32 devices in a mesh: sp: 8 (over z, x), tp: 4 (over y, core).
Axes of the slice: x: 2, y: 2, z: 4, core: 2. Of those that a mesh axis runs over, the one named last changes fastest.
Arguments:
- stream: bfloat16 [4096, 2048], P(('sp', 'tp')), may hold values from -6 to 6
- queries: bfloat16 [4096, 512], P('sp', 'tp'), may hold values from -6 to 6
- key_rows: bfloat16 [4096, 512], P('sp', 'tp'), may hold values from -6 to 6
- values: bfloat16 [4096, 1024], P('sp', 'tp'), may hold values from -6 to 6
- out_gate: bfloat16 [4096, 1024], P('sp', 'tp'), may hold values from -6 to 6
- fwd_decay: float32 [4096, 512], P('sp', 'tp'), may hold values from -14 to 14
- bwd_decay: float32 [4096, 512], P('sp', 'tp'), may hold values from -14 to 14
- head_gain: float32 [1024], P('tp'), may hold values from 0.1 to 1.9
- out_proj: bfloat16 [1024, 2048], replicated, may hold values from -0.1875 to 0.1875
- mix_gain: float32 [2048], replicated, may hold values from 0.1 to 1.9
- ffn_gain: float32 [2048], replicated, may hold values from 0.1 to 1.9
- moe_gain: float32 [2048], replicated, may hold values from 0.1 to 1.9
- routes: int32 [4096, 2], P(('sp', 'tp')), may hold values from 0 to 7, all different within a row; in each aligned block of 128 rows (0 to 127, 128 to 255, ...) at most 48 rows name the same one
- route_weight: float32 [4096, 2], P(('sp', 'tp')), may hold values from 0.25 to 2.5
- expert_gate: bfloat16 [8, 2048, 1024], P('sp', None, 'tp'), may hold values from -0.125 to 0.125
- expert_up: bfloat16 [8, 2048, 1024], P('sp', None, 'tp'), may hold values from -0.125 to 0.125
- expert_down: bfloat16 [8, 1024, 2048], P('sp', 'tp'), may hold values from -0.1875 to 0.1875
- shared_gate: bfloat16 [2048, 512], P(None, 'tp'), may hold values from -0.125 to 0.125
- shared_up: bfloat16 [2048, 512], P(None, 'tp'), may hold values from -0.125 to 0.125
- shared_down: bfloat16 [512, 2048], P('tp'), may hold values from -0.25 to 0.25
Outputs:
- updated: bfloat16 [4096, 2048], P(('sp', 'tp'))
The draws below stay inside these ranges and needn't reach their ends.
Inputs may be any that keep to these rules, and one draw needn't show every extreme that they name: `routes`: each row names 2 different experts. Among the rows of one device no expert is named more than 48 times, and in every draw some device names some expert exactly 48 times.
All inputs are finite; a program needn't handle non-finite values.
Results may differ from the reference program's by a relative error of at most 0.023.
Values may be sent and summed in bfloat16 or wider, within the bound.
A program may use at most 128 MiB of HBM per device.

```python
import math
import jax
import jax.numpy as jnp
import numpy as np
from jax import lax

D = 2048
HEAD_TOTAL = 8
KEY_CHANNELS = 64
DV = 128
BLK = 64
FE = 1024
SH = 512
TOPK = 2
TOK_DEV = 128
TOKEN_COUNT = 4096
HV = 1024
EXPERTS = 8
CAP = 48
PARTS_SIZE = 4


def decay_law(key):
    head_key, chan_key, dev_key, jitter_key, position_key, fraction_key = jax.random.split(key, 6)
    slow_share = 0.5
    slow_heads = jax.random.uniform(head_key, (HEAD_TOTAL,)) < slow_share
    head_rate = jnp.where(slow_heads, 0.6 / TOKEN_COUNT, 2.5 / BLK)
    channel_rate = jnp.repeat(head_rate, KEY_CHANNELS) * jnp.exp(jax.random.uniform(chan_key, (HEAD_TOTAL * KEY_CHANNELS,), minval=-0.5, maxval=0.5))
    device_factor = jnp.exp(jax.random.uniform(dev_key, (TOKEN_COUNT // TOK_DEV, 1), minval=-0.7, maxval=0.7))
    rates = jnp.repeat(device_factor, TOK_DEV, axis=0) * channel_rate[None, :]
    preactivation = -jnp.log(jnp.expm1(16.0 * rates))
    preactivation = preactivation + jax.random.uniform(jitter_key, (TOKEN_COUNT, HEAD_TOTAL * KEY_CHANNELS), minval=-1.0, maxval=1.0)
    spike_rows = jax.random.randint(position_key, (2,), 0, TOKEN_COUNT)
    spike_fraction = jax.random.uniform(fraction_key, (2, HEAD_TOTAL * KEY_CHANNELS), minval=0.2, maxval=0.5)
    spike_preactivation = -jnp.log(jnp.expm1(-16.0 * jnp.log(1.0 - spike_fraction)))
    preactivation = preactivation.at[spike_rows].set(spike_preactivation)
    return jnp.clip(preactivation, -14.0, 14.0).astype(jnp.float32)


def draw_fwd_decay(key, part):
    return decay_law(jax.random.fold_in(key, 11))


def draw_bwd_decay(key, part):
    return decay_law(jax.random.fold_in(key, 23))


def levels(own_key, dims, cuts, low, high):
    gain = 1.0
    for dim, blocks in cuts:
        draws = jax.random.uniform(jax.random.fold_in(jax.random.fold_in(own_key, 6), dim), (blocks,), jnp.float32, low / len(cuts), high / len(cuts))
        gain = gain * jnp.repeat(jnp.exp(draws), dims[dim] // blocks).reshape((-1,) + (1,) * (len(dims) - 1 - dim))
    return gain


def deal_out(key, own, number, rows, amount, top, most, lean):
    sequence = jax.random.permutation(key, amount)
    heavy_load, ordinary = portions_of(amount, rows * top, most, lean, True), portions_of(amount, rows * top, most, lean, False)
    places = jnp.arange(amount)

    def named(tallies, rotation):
        used = int((tallies > 0).sum())
        fixed = max(1, used // 4)
        shifted = fixed + (places - fixed + rotation * (used - fixed)) % max(1, amount - fixed)
        return jnp.zeros((amount,), jnp.int32).at[sequence[jnp.where(places < fixed, places, shifted)]].set(jnp.asarray(tallies, jnp.int32))

    tallies = jnp.where(number % 4 == 0, named(heavy_load, number // 4), named(ordinary, number - number // 4 - 1))
    mixed = jax.random.permutation(jax.random.fold_in(own, 3), amount)
    giver, taker = mixed[0:amount // 2 * 2:2], mixed[1:amount // 2 * 2:2]
    room = jnp.minimum(tallies[giver] - 1, most - tallies[taker]) // 2
    room = jnp.where((giver == sequence[0]) | (taker == sequence[0]) | (tallies[taker] == 0), 0, jnp.maximum(room, 0))
    shifted = jax.random.randint(jax.random.fold_in(own, 4), (amount // 2,), 0, 1 << 20) % (room + 1)
    tallies = tallies.at[giver].add(-shifted).at[taker].add(shifted)
    members = jnp.searchsorted(jnp.cumsum(tallies), jnp.arange(rows * top), side="right").astype(jnp.int32)
    listing = members.reshape(top, rows).T
    listing = listing[jax.random.permutation(jax.random.fold_in(own, 1), rows)]
    rotation = jax.random.randint(jax.random.fold_in(own, 2), (rows, 1), 0, top)
    return jnp.take_along_axis(listing, (jnp.arange(top)[None, :] + rotation) % top, axis=1)


def portions_of(count, total, reach, skew, full):
    weights = [(1 << 20) // math.isqrt(standing ** skew) + 1 for standing in range(1, count + 1)]
    largest = reach if full else min(reach, max(-(-total // count), total * weights[0] // sum(weights)))
    least = 1 if total - largest >= count - 1 else 0
    given, surplus = [largest] + [least] * (count - 1), total - largest - least * (count - 1)
    while surplus > 0:
        free = [i for i in range(1, count) if given[i] < largest] or [i for i in range(1, count) if given[i] < reach]
        mass, left = sum([weights[i] for i in free]), surplus
        for i in free:
            extra = min(reach - given[i], max(1, left * weights[i] // mass), surplus)
            given[i] = given[i] + extra
            surplus = surplus - extra
    return np.array(given)


def bell_draw(own_key, dims, width, most, cuts=(), kind=jnp.bfloat16):
    drawn = jax.random.normal(own_key, dims, jnp.float32) * width
    if len(cuts) > 0:
        drawn = levels(own_key, dims, cuts, -0.22, 0.18) * drawn
    return jnp.clip(drawn, min=-most, max=most).astype(kind)


def setup_inputs(seed: int = 0) -> dict:
    arg_keys = jax.random.split(jax.random.key(seed), 21)
    stream = bell_draw(arg_keys[0], (TOKEN_COUNT, D), 1.0, 6.0, ((0, 32),))
    queries = bell_draw(arg_keys[1], (TOKEN_COUNT, HEAD_TOTAL * KEY_CHANNELS), 1.0, 6.0, ((0, 8), (1, 4)))
    key_rows = bell_draw(arg_keys[2], (TOKEN_COUNT, HEAD_TOTAL * KEY_CHANNELS), 1.0, 6.0, ((0, 8), (1, 4)))
    values = bell_draw(arg_keys[3], (TOKEN_COUNT, HV), 1.0, 6.0, ((0, 8), (1, 4)))
    out_gate = bell_draw(arg_keys[4], (TOKEN_COUNT, HV), 1.0, 6.0, ((0, 8), (1, 4)))
    fwd_decay = draw_fwd_decay(jax.random.fold_in(arg_keys[20], 71), 0)
    bwd_decay = draw_bwd_decay(jax.random.fold_in(arg_keys[20], 71), 0)
    head_gain = jnp.clip(1.0 + 0.18 * jax.random.normal(arg_keys[7], (HV,), jnp.float32), 0.1, 1.9)
    out_proj = bell_draw(arg_keys[8], (HV, D), HV ** -0.5, 0.1875)
    mix_gain = jnp.clip(1.0 + 0.18 * jax.random.normal(arg_keys[9], (D,), jnp.float32), 0.1, 1.9)
    ffn_gain = jnp.clip(1.0 + 0.18 * jax.random.normal(arg_keys[10], (D,), jnp.float32), 0.1, 1.9)
    moe_gain = jnp.clip(1.0 + 0.18 * jax.random.normal(arg_keys[11], (D,), jnp.float32), 0.1, 1.9)
    routes_keys = jax.random.split(jax.random.fold_in(arg_keys[12], 1), TOKEN_COUNT // TOK_DEV)
    routes_turns = jax.random.permutation(jax.random.fold_in(arg_keys[12], 3), TOKEN_COUNT // TOK_DEV)
    routes = jax.vmap(lambda own, number: deal_out(jax.random.fold_in(arg_keys[12], 2), own, number, TOK_DEV, EXPERTS, TOPK, CAP, 1))(routes_keys, routes_turns).reshape((TOKEN_COUNT, TOPK))
    route_weight = jnp.clip(jnp.exp(math.log(2.5) - 2.3025851 * jax.random.uniform(arg_keys[13], (TOKEN_COUNT, TOPK), jnp.float32) ** levels(arg_keys[13], (TOKEN_COUNT, TOPK), ((0, 32),), -0.2, 0.2)), 0.25, 2.5)
    expert_gate = bell_draw(arg_keys[14], (EXPERTS, D, FE), D ** -0.5, 0.125, ((0, 8), (2, 4)))
    expert_up = bell_draw(arg_keys[15], (EXPERTS, D, FE), D ** -0.5, 0.125, ((0, 8), (2, 4)))
    expert_down = bell_draw(arg_keys[16], (EXPERTS, FE, D), FE ** -0.5, 0.1875, ((0, 8), (1, 4)))
    shared_gate = bell_draw(arg_keys[17], (D, SH), D ** -0.5, 0.125, ((1, 4),))
    shared_up = bell_draw(arg_keys[18], (D, SH), D ** -0.5, 0.125, ((1, 4),))
    shared_down = bell_draw(arg_keys[19], (SH, D), SH ** -0.5, 0.25, ((0, 4),))
    return {"stream": stream, "queries": queries, "key_rows": key_rows, "values": values, "out_gate": out_gate, "fwd_decay": fwd_decay, "bwd_decay": bwd_decay, "head_gain": head_gain, "out_proj": out_proj, "mix_gain": mix_gain, "ffn_gain": ffn_gain, "moe_gain": moe_gain, "routes": routes, "route_weight": route_weight, "expert_gate": expert_gate, "expert_up": expert_up, "expert_down": expert_down, "shared_gate": shared_gate, "shared_up": shared_up, "shared_down": shared_down}


EPS = 1e-06
GATE_NORM = 16.0
ROPE_BASE = 10000.0
TOP_PRECISION = lax.Precision.HIGHEST

def normalize(tensor):
    return tensor * lax.rsqrt(lax.optimization_barrier(jnp.mean(tensor * tensor, axis=-1, keepdims=True)) + EPS)

def rotate(tensor, positions):
    half_width = tensor.shape[-1] // 2
    frequency = ROPE_BASE ** (-jnp.arange(half_width, dtype=jnp.float32) / half_width)
    angles = positions[:, None] * frequency[None, :]
    cosine = jnp.cos(angles)[:, None, :]
    sine_part = jnp.sin(angles)[:, None, :]
    front_half = tensor[..., :half_width]
    back_half = tensor[..., half_width:]
    return jnp.concatenate([front_half * cosine - back_half * sine_part, front_half * sine_part + back_half * cosine], axis=-1)

def blockwise(query_rows, key_data, value_matrix, log_decay, start_state):
    length, head_count, key_width = query_rows.shape
    value_width = value_matrix.shape[-1]
    block_count = length // BLK
    query_blocks = query_rows.reshape(block_count, BLK, head_count, key_width)
    key_blocks = key_data.reshape(block_count, BLK, head_count, key_width)
    value_blocks = value_matrix.reshape(block_count, BLK, head_count, value_width)
    cumul = jnp.cumsum(log_decay.reshape(block_count, BLK, head_count, key_width), axis=1)
    middle = cumul[:, BLK // 2 - 1:BLK // 2]
    query_scaled = query_blocks * jnp.exp(cumul - middle)
    key_scaled = key_blocks * jnp.exp(middle - cumul)
    scores = jnp.einsum('nthk,nshk->nhts', query_scaled, key_scaled, precision=TOP_PRECISION)
    lower_mask = jnp.arange(BLK)[:, None] >= jnp.arange(BLK)[None, :]
    scores = jnp.where(lower_mask, scores, 0.0)
    within = jnp.einsum('nhts,nshv->nthv', scores, value_blocks, precision=TOP_PRECISION)
    last_cumul = cumul[:, -1:]
    query_in = query_blocks * jnp.exp(cumul)
    key_out = key_blocks * jnp.exp(last_cumul - cumul)
    block_decay = jnp.exp(last_cumul[:, 0])

    def advance(carried_state, pieces):
        query_segment, key_segment, value_segment, decay_segment = pieces
        across_blocks = jnp.einsum('asu,sun->asn', query_segment, carried_state, precision=TOP_PRECISION)
        carried_state = carried_state * decay_segment[:, :, None] + jnp.einsum('jco,jcm->com', key_segment, value_segment, precision=TOP_PRECISION)
        return (carried_state, across_blocks)
    final_state, across_blocks = lax.scan(advance, start_state, (query_in, key_out, value_blocks, block_decay))
    return ((within + across_blocks).reshape(length, head_count, value_width), final_state)

def reference(stream, queries, key_rows, values, out_gate, fwd_decay, bwd_decay, head_gain, out_proj, mix_gain, ffn_gain, moe_gain, routes, route_weight, expert_gate, expert_up, expert_down, shared_gate, shared_up, shared_down):
    positions = jnp.arange(TOKEN_COUNT, dtype=jnp.int32).astype(jnp.float32)
    query_rows = rotate(queries.astype(jnp.float32).reshape(TOKEN_COUNT, HEAD_TOTAL, KEY_CHANNELS) * KEY_CHANNELS ** (-0.5), positions)
    key_data = rotate(key_rows.astype(jnp.float32).reshape(TOKEN_COUNT, HEAD_TOTAL, KEY_CHANNELS), positions)
    value_matrix = values.astype(jnp.float32).reshape(TOKEN_COUNT, HEAD_TOTAL, DV)
    fwd_log = jax.nn.log_sigmoid(fwd_decay).reshape(TOKEN_COUNT, HEAD_TOTAL, KEY_CHANNELS) / GATE_NORM
    bwd_log = jax.nn.log_sigmoid(bwd_decay).reshape(TOKEN_COUNT, HEAD_TOTAL, KEY_CHANNELS) / GATE_NORM
    zero_state = jnp.zeros((HEAD_TOTAL, KEY_CHANNELS, DV), jnp.float32)
    fwd_out, _ = blockwise(query_rows, key_data, value_matrix, fwd_log, zero_state)
    bwd_out, _ = blockwise(query_rows[::-1], key_data[::-1], value_matrix[::-1], bwd_log[::-1], zero_state)
    combined = normalize(fwd_out + bwd_out[::-1]) * head_gain.reshape(HEAD_TOTAL, DV)
    mixed_out = (combined.reshape(TOKEN_COUNT, HV) * jax.nn.silu(out_gate.astype(jnp.float32))).astype(jnp.bfloat16)
    projected = jnp.dot(mixed_out, out_proj, preferred_element_type=jnp.float32)
    residual = (stream.astype(jnp.float32) + normalize(projected) * mix_gain).astype(jnp.bfloat16)
    normed = (normalize(residual.astype(jnp.float32)) * ffn_gain).astype(jnp.bfloat16)
    shared_hidden = (jax.nn.silu(jnp.dot(normed, shared_gate, preferred_element_type=jnp.float32)) * jnp.dot(normed, shared_up, preferred_element_type=jnp.float32)).astype(jnp.bfloat16)
    group_width = SH // PARTS_SIZE
    shared_out = jnp.zeros((TOKEN_COUNT, D), jnp.float32)
    for quarter in range(PARTS_SIZE):
        piece = jnp.dot(shared_hidden[:, quarter * group_width:(quarter + 1) * group_width], shared_down[quarter * group_width:(quarter + 1) * group_width], preferred_element_type=jnp.float32)
        shared_out = shared_out + lax.optimization_barrier(piece.astype(jnp.bfloat16)).astype(jnp.float32)
    row_block = 256
    flat_ids = routes.reshape(-1)
    grand_total = flat_ids.shape[0]
    token_index = jnp.arange(grand_total, dtype=jnp.int32) // TOPK
    sort_order = jnp.argsort(flat_ids, stable=True)
    sorted_expert = flat_ids[sort_order]
    sorted_token = token_index[sort_order]
    sorted_weight = route_weight.reshape(-1)[sort_order]
    counts = lax.optimization_barrier(jnp.sum((flat_ids[:, None] == jnp.arange(EXPERTS, dtype=jnp.int32)[None, :]).astype(jnp.int32), axis=0))
    starts = jnp.cumsum(counts) - counts
    padded = (counts + row_block - 1) // row_block * row_block
    block_ends = jnp.cumsum(padded)
    padded_starts = block_ends - padded
    position = (padded_starts[sorted_expert] + jnp.arange(grand_total, dtype=jnp.int32) - starts[sorted_expert]).astype(jnp.int32)
    block_total = -(-(grand_total + EXPERTS * (row_block - 1)) // row_block)
    slot_token = jnp.zeros((block_total * row_block,), jnp.int32).at[position].set(sorted_token)
    slot_weight = jnp.zeros((block_total * row_block,), jnp.float32).at[position].set(sorted_weight)
    block_expert = jnp.minimum(jnp.searchsorted(block_ends, jnp.arange(block_total, dtype=jnp.int32) * row_block, side='right'), EXPERTS - 1).astype(jnp.int32)
    expert_width = FE // PARTS_SIZE

    def add_block(totals, block_item):
        token_ids, slot_wts, expert = block_item
        row_data = normed[token_ids]
        gate_mat = lax.dynamic_index_in_dim(expert_gate, expert, 0, keepdims=False)
        up_mat = lax.dynamic_index_in_dim(expert_up, expert, 0, keepdims=False)
        down_mat = lax.dynamic_index_in_dim(expert_down, expert, 0, keepdims=False)
        hidden = (jax.nn.silu(jnp.dot(row_data, gate_mat, preferred_element_type=jnp.float32)) * jnp.dot(row_data, up_mat, preferred_element_type=jnp.float32)).astype(jnp.bfloat16)
        quarter_sums = jnp.einsum('rqf,qfd->qrd', hidden.astype(jnp.float32).reshape(row_block, PARTS_SIZE, expert_width), down_mat.astype(jnp.float32).reshape(PARTS_SIZE, expert_width, D), precision=TOP_PRECISION)
        rounded = lax.optimization_barrier(quarter_sums.astype(jnp.bfloat16)).astype(jnp.float32)
        result = lax.optimization_barrier(lax.optimization_barrier(jnp.sum(rounded, axis=0)).astype(jnp.bfloat16)).astype(jnp.float32)
        return (totals.at[token_ids].add(result * slot_wts[:, None]), None)
    routed_sum, _ = lax.scan(add_block, jnp.zeros((TOKEN_COUNT, D), jnp.float32), (slot_token.reshape(block_total, row_block), slot_weight.reshape(block_total, row_block), block_expert))
    mixture = shared_out + routed_sum
    return (residual.astype(jnp.float32) + normalize(mixture) * moe_gain).astype(jnp.bfloat16)
```

```python
import functools

import jax
import jax.numpy as jnp
from jax import lax
from jax.experimental import pallas as pl
from jax.experimental.pallas import tpu as pltpu
from jax.sharding import PartitionSpec as P

KEY_CHANNELS = 64
DV = 128
BLK = 64
TOPK = 2
ROW_TILE = 16


EPS = 1e-06
GATE_NORM = 16.0
ROPE_BASE = 10000.0
MESH = pl.DeviceIdType.MESH
WEIGHT_CUTS = 4
WEIGHT_EARLY = 4


def dot_nn(left, right):
    return jnp.dot(left, right, preferred_element_type=jnp.float32)


def dot_nt(left, right):
    return lax.dot_general(
        left, right, (((1,), (1,)), ((), ())), preferred_element_type=jnp.float32
    )


def dot_tn(left, right):
    return lax.dot_general(
        left, right, (((0,), (0,)), ((), ())), preferred_element_type=jnp.float32
    )


def layer_kernel(
    sp_count,
    tp_count,
    capacity,
    return_cuts,
    q_ref,
    k_ref,
    v_ref,
    fwd_ref,
    bwd_ref,
    table_ref,
    gain_ref,
    mix_gain_ref,
    ffn_gain_ref,
    moe_gain_ref,
    routes_ref,
    route_weight_ref,
    out_gate_hbm,
    stream_hbm,
    proj_hbm,
    gate_hbm,
    up_hbm,
    down_hbm,
    shared_gate_hbm,
    shared_up_hbm,
    shared_down_hbm,
    out_ref,
    out_gate_ref,
    stream_ref,
    proj_ref,
    gate_ref,
    up_ref,
    down_ref,
    sgate_ref,
    sup_ref,
    sdown_ref,
    own_ref,
    got_ref,
    mixed_ref,
    land_ref,
    within_ref,
    key_ref,
    sums_f,
    sums_b,
    heads_ref,
    wide_ref,
    residual_ref,
    normed_ref,
    outgoing_ref,
    arrived_ref,
    hidden_ref,
    done_ref,
    back_ref,
    local_sem,
    sum_send,
    sum_recv,
    row_send,
    row_recv,
    block_send,
    block_recv,
    back_send,
    back_recv,
    weight_sem,
    pair_send,
    pair_recv,
    cross_send,
    cross_recv,
    relay_send,
    relay_recv,
    near_send,
    near_recv,
    slice_send,
    slice_recv,
    spread_send,
    spread_recv,
    side_send,
    side_recv,
    last_send,
    last_recv,
):
    span, lanes = q_ref.shape
    width = v_ref.shape[1]
    heads = lanes // KEY_CHANNELS
    blocks = span // BLK
    tokens = span // tp_count
    model = stream_ref.shape[1]
    part_width = gate_ref.shape[2]
    slots = sp_count * capacity
    cut = model // return_cuts
    piece = model // WEIGHT_CUTS
    sp_me = lax.axis_index("sp")
    tp_me = lax.axis_index("tp")
    ranks = tp_count // 2
    rank = lax.div(tp_me, 2)
    seat = lax.rem(tp_me, 2)
    buddy = (sp_me, tp_me + 1 - 2 * seat)
    team = min(8, sp_count)
    place = lax.rem(sp_me, team)
    team_base = sp_me - place
    sends = []

    def sp_peer(step):
        return (lax.rem(sp_me + step, sp_count), tp_me)

    def tp_peer(step):
        return (sp_me, lax.rem(tp_me + step, tp_count))

    def cross_tp(step):
        return lax.rem(rank + step, ranks) * 2 + seat

    def send(source, target, send_sem, recv_sem, device):
        copy = pltpu.make_async_remote_copy(
            src_ref=source,
            dst_ref=target,
            send_sem=send_sem,
            recv_sem=recv_sem,
            device_id=device,
            device_id_type=MESH,
        )
        copy.start()
        sends.append(copy)
        return copy

    def fetch(source, target, semaphore):
        copy = pltpu.make_async_copy(source, target, semaphore)
        copy.start()
        return copy

    barrier = pltpu.get_barrier_semaphore()
    for step in range(1, sp_count):
        pl.semaphore_signal(barrier, inc=1, device_id=sp_peer(step), device_id_type=MESH)
    for step in range(1, tp_count):
        pl.semaphore_signal(barrier, inc=1, device_id=tp_peer(step), device_id_type=MESH)

    def weight_source(index):
        kind, at = divmod(index, WEIGHT_CUTS)
        if kind < 2:
            return (gate_hbm, up_hbm)[kind].at[0, pl.ds(at * piece, piece), :]
        return down_hbm.at[0, :, pl.ds(at * piece, piece)]

    def weight_slot(index, owner):
        kind, at = divmod(index, WEIGHT_CUTS)
        if kind < 2:
            return (gate_ref, up_ref)[kind].at[owner, pl.ds(at * piece, piece), :]
        row = pl.multiple_of(owner * part_width, part_width)
        return down_ref.at[at, pl.ds(row, part_width), :]

    shared_lanes = shared_gate_hbm.shape[1]

    def shared_slot(kind, owner, which=None):
        column = pl.ds(pl.multiple_of(owner * shared_lanes, shared_lanes), shared_lanes)
        if kind < 2:
            ref = (sgate_ref, sup_ref)[kind]
            if which is None:
                return ref.at[:, column]
            size = model // team
            return ref.at[pl.ds(pl.multiple_of(which * size, size), size), column]
        if which is None:
            return sdown_ref.at[column, :]
        size = shared_lanes // team
        row = pl.multiple_of(owner * shared_lanes + which * size, size)
        return sdown_ref.at[pl.ds(row, size), :]

    def shared_source(kind, which=None):
        ref = (shared_gate_hbm, shared_up_hbm, shared_down_hbm)[kind]
        if which is None:
            return ref
        size = (shared_lanes if kind == 2 else model) // team
        return ref.at[pl.ds(pl.multiple_of(which * size, size), size), :]

    count = 3 * WEIGHT_CUTS
    gate_fetch = fetch(out_gate_hbm, out_gate_ref, local_sem.at[0])
    stream_fetch = fetch(stream_hbm, stream_ref, local_sem.at[1])
    proj_fetch = fetch(proj_hbm, proj_ref, local_sem.at[2])
    shared_fetches = [
        fetch(shared_source(kind), shared_slot(kind, tp_me), local_sem.at[3 + kind])
        for kind in range(3)
    ]
    weight_fetches = [
        fetch(weight_source(index), weight_slot(index, tp_me), weight_sem.at[index])
        for index in range(count)
    ]

    row = lax.broadcasted_iota(jnp.int32, (BLK, BLK), 0)
    column = lax.broadcasted_iota(jnp.int32, (BLK, BLK), 1)
    lower = row >= column
    upper = row <= column
    lower_ones = lower.astype(jnp.bfloat16)
    upper_ones = upper.astype(jnp.bfloat16)
    from_lane = lax.broadcasted_iota(jnp.int32, (lanes, lanes), 0)
    to_lane = lax.broadcasted_iota(jnp.int32, (lanes, lanes), 1)
    half = KEY_CHANNELS // 2
    partner = jnp.where(lax.rem(to_lane, KEY_CHANNELS) < half, to_lane + half, to_lane - half)
    swap = (from_lane == partner).astype(jnp.bfloat16)
    own_head = (
        lax.broadcasted_iota(jnp.int32, (width, lanes), 0) // DV
        == lax.broadcasted_iota(jnp.int32, (width, lanes), 1) // KEY_CHANNELS
    )
    lane_head = lax.broadcasted_iota(jnp.int32, (BLK, lanes), 1) // KEY_CHANNELS

    cos_row, sin_row = table_ref[0, 0:BLK, :], table_ref[1, 0:BLK, :]

    def rotated(tensor, block):
        cos_at = table_ref[0, BLK + block : BLK + block + 1, :]
        sin_at = table_ref[1, BLK + block : BLK + block + 1, :]
        cosine = cos_row * cos_at - sin_row * sin_at
        sine = sin_row * cos_at + cos_row * sin_at
        return tensor.astype(jnp.float32) * cosine + dot_nn(tensor, swap) * sine

    def running(ones, raw):
        logs = (jnp.minimum(raw, 0.0) - jnp.log1p(jnp.exp(-jnp.abs(raw)))) * (1.0 / GATE_NORM)
        first = logs.astype(jnp.bfloat16)
        rest = logs - first.astype(jnp.float32)
        second = rest.astype(jnp.bfloat16)
        third = (rest - second.astype(jnp.float32)).astype(jnp.bfloat16)
        return dot_nn(ones, first) + (dot_nn(ones, second) + dot_nn(ones, third))

    pl.semaphore_wait(barrier, sp_count - 1 + tp_count - 1)

    near, slices = [], []
    for kind in range(3):
        for step in range(1, ranks):
            slices.append(
                send(
                    shared_source(kind, place),
                    shared_slot(kind, tp_me, place),
                    slice_send.at[step, kind],
                    slice_recv.at[step, kind],
                    (sp_me, cross_tp(step)),
                )
            )

    crossings = {}

    def cross(index):
        crossings[index] = [
            send(
                weight_source(index),
                weight_slot(index, tp_me),
                cross_send.at[step, index],
                cross_recv.at[step, index],
                (sp_me, cross_tp(step)),
            )
            for step in range(1, ranks)
        ]

    relays = {}

    def relay(index):
        relays[index] = []
        for step in range(1, ranks):
            crossings[index][step - 1].wait_recv()
            owner = lax.rem(rank + ranks - step, ranks) * 2 + seat
            relays[index].append(
                send(
                    weight_slot(index, owner),
                    weight_slot(index, owner),
                    relay_send.at[step, index],
                    relay_recv.at[step, index],
                    buddy,
                )
            )

    cross(0)
    cross(1)
    for kind in range(3):
        near.append(
            send(
                shared_source(kind),
                shared_slot(kind, tp_me),
                near_send.at[kind],
                near_recv.at[kind],
                buddy,
            )
        )
    pairs = [
        send(
            weight_source(index),
            weight_slot(index, tp_me),
            pair_send.at[index],
            pair_recv.at[index],
            buddy,
        )
        for index in range(count)
    ]

    cumul_f, cumul_b, decay_f, decay_b = [], [], [], []
    for block in range(blocks):
        rows = pl.ds(block * BLK, BLK)
        total_f = running(lower_ones, fwd_ref[rows, :])
        total_b = running(upper_ones, bwd_ref[rows, :])
        last_f = total_f[BLK - 1 : BLK]
        last_b = total_b[0:1]
        keys = rotated(k_ref[rows, :], block)
        key_ref[rows, :] = keys
        value_rows = v_ref[rows, :]
        out_f = (keys * jnp.exp(last_f - total_f)).astype(jnp.bfloat16)
        out_b = (keys * jnp.exp(last_b - total_b)).astype(jnp.bfloat16)
        sums_f[block] = jnp.where(own_head, dot_tn(value_rows, out_f), 0.0)
        sums_b[block] = jnp.where(own_head, dot_tn(value_rows, out_b), 0.0)
        cumul_f.append(total_f)
        cumul_b.append(total_b)
        decay_f.append(jnp.exp(last_f))
        decay_b.append(jnp.exp(last_b))

    def packed(total):
        return sum(total[h * DV : (h + 1) * DV] for h in range(heads))

    total = sums_f[0]
    through = decay_f[0]
    for block in range(1, blocks):
        total = total * decay_f[block] + sums_f[block]
        through = through * decay_f[block]
    own_ref[0, 0:DV, :] = packed(total).astype(jnp.bfloat16)
    own_ref[0, DV : DV + 16, :] = jnp.broadcast_to(through, (16, lanes)).astype(jnp.bfloat16)
    total = sums_b[blocks - 1]
    through = decay_b[blocks - 1]
    for block in range(blocks - 2, -1, -1):
        total = total * decay_b[block] + sums_b[block]
        through = through * decay_b[block]
    own_ref[1, 0:DV, :] = packed(total).astype(jnp.bfloat16)
    own_ref[1, DV : DV + 16, :] = jnp.broadcast_to(through, (16, lanes)).astype(jnp.bfloat16)

    sum_copies = [
        send(
            own_ref.at[lax.div(sp_me + step, sp_count)],
            got_ref.at[step],
            sum_send.at[step],
            sum_recv.at[step],
            sp_peer(step),
        )
        for step in range(1, sp_count)
    ]
    cross(2)

    spreads = []
    for copy in slices:
        copy.wait_recv()
    for hop in range(1, team // 2):
        to_place = lax.rem(place + 2 * hop, team)
        for step in range(1, ranks):
            owner = lax.rem(rank + ranks - step, ranks) * 2 + seat
            for kind in range(3):
                spreads.append(
                    send(
                        shared_slot(kind, owner, place),
                        shared_slot(kind, owner, place),
                        spread_send.at[hop, step, kind],
                        spread_recv.at[hop, step, kind],
                        (team_base + to_place, tp_me),
                    )
                )

    query_f, query_b = [], []
    for block in range(blocks):
        rows = pl.ds(block * BLK, BLK)
        queries = rotated(q_ref[rows, :], block) * KEY_CHANNELS ** (-0.5)
        keys = key_ref[rows, :]
        total_f, total_b = cumul_f[block], cumul_b[block]
        middle_f = total_f[BLK // 2 - 1 : BLK // 2]
        middle_b = total_b[BLK // 2 : BLK // 2 + 1]
        scaled_qf = queries * jnp.exp(total_f - middle_f)
        scaled_qb = queries * jnp.exp(total_b - middle_b)
        scaled_kf = (keys * jnp.exp(middle_f - total_f)).astype(jnp.bfloat16)
        scaled_kb = (keys * jnp.exp(middle_b - total_b)).astype(jnp.bfloat16)
        query_f.append((queries * jnp.exp(total_f)).astype(jnp.bfloat16))
        query_b.append((queries * jnp.exp(total_b)).astype(jnp.bfloat16))
        for h in range(heads):
            mine = lane_head == h
            scores_f = dot_nt(jnp.where(mine, scaled_qf, 0.0).astype(jnp.bfloat16), scaled_kf)
            scores_b = dot_nt(jnp.where(mine, scaled_qb, 0.0).astype(jnp.bfloat16), scaled_kb)
            scores = jnp.where(lower, scores_f, 0.0) + jnp.where(upper, scores_b, 0.0)
            within_ref[rows, h * DV : (h + 1) * DV] = dot_nn(
                scores.astype(jnp.bfloat16), v_ref[rows, h * DV : (h + 1) * DV]
            )
    for index in range(3, WEIGHT_EARLY):
        cross(index)

    for copy in sum_copies:
        copy.wait_recv()
    carry_f = jnp.zeros((DV, lanes), jnp.float32)
    carry_b = jnp.zeros((DV, lanes), jnp.float32)
    for step in range(sp_count - 1, 0, -1):
        state = got_ref[step, 0:DV, :].astype(jnp.float32)
        through = got_ref[step, DV : DV + 16, :].astype(jnp.float32)[0:1]
        carry_f = jnp.where(step <= sp_me, carry_f * through + state, carry_f)
    for step in range(1, sp_count):
        state = got_ref[step, 0:DV, :].astype(jnp.float32)
        through = got_ref[step, DV : DV + 16, :].astype(jnp.float32)[0:1]
        carry_b = jnp.where(step > sp_me, carry_b * through + state, carry_b)

    def unpacked(carry):
        return jnp.where(own_head, jnp.concatenate([carry] * heads, axis=0), 0.0)

    state = unpacked(carry_f)
    for block in range(blocks):
        rows = pl.ds(block * BLK, BLK)
        within_ref[rows, :] += dot_nt(query_f[block], state.astype(jnp.bfloat16))
        if block < blocks - 1:
            state = state * decay_f[block] + sums_f[block]
    gate_fetch.wait()
    state = unpacked(carry_b)
    for block in range(blocks - 1, -1, -1):
        rows = pl.ds(block * BLK, BLK)
        attended = within_ref[rows, :] + dot_nt(query_b[block], state.astype(jnp.bfloat16))
        if block > 0:
            state = state * decay_b[block] + sums_b[block]
        for h in range(heads):
            part = attended[:, h * DV : (h + 1) * DV]
            square = jnp.mean(part * part, axis=-1, keepdims=True)
            gate = out_gate_ref[rows, h * DV : (h + 1) * DV].astype(jnp.float32)
            mixed_ref[rows, h * DV : (h + 1) * DV] = (
                part
                * lax.rsqrt(square + EPS)
                * gain_ref[:, h * DV : (h + 1) * DV]
                * (gate / (1.0 + jnp.exp(-gate)))
            ).astype(jnp.bfloat16)

    row_copies = []
    for step in range(1, tp_count):
        target = lax.rem(tp_me + step, tp_count)
        row_copies.append(
            send(
                mixed_ref.at[pl.ds(pl.multiple_of(target * tokens, tokens), tokens)],
                land_ref.at[tp_me],
                row_send.at[step],
                row_recv.at[step],
                (sp_me, target),
            )
        )
    for index in range(WEIGHT_EARLY, count):
        cross(index)
    land_ref[tp_me] = mixed_ref[pl.ds(pl.multiple_of(tp_me * tokens, tokens), tokens), :]

    token_row = lax.broadcasted_iota(jnp.int32, (tokens, tokens), 0)
    token_column = lax.broadcasted_iota(jnp.int32, (tokens, tokens), 1)
    earlier = (token_row > token_column).astype(jnp.bfloat16)
    expert_lane = lax.broadcasted_iota(jnp.int32, (tokens, 128), 1)
    choices = [routes_ref[:, choice : choice + 1] for choice in range(TOPK)]
    named = [(chosen == expert_lane).astype(jnp.float32) for chosen in choices]
    before = dot_nn(earlier, sum(named).astype(jnp.bfloat16))
    slot_lane = lax.broadcasted_iota(jnp.int32, (tokens, slots), 1).astype(jnp.float32)
    weights = jnp.zeros((tokens, slots), jnp.float32)
    picked = jnp.zeros((tokens, slots), jnp.float32)
    for choice in range(TOPK):
        slot = jnp.sum(before * named[choice], axis=1, keepdims=True)
        place_of = choices[choice].astype(jnp.float32) * capacity + slot
        hit = slot_lane == place_of
        picked = jnp.where(hit, 1.0, picked)
        weights = jnp.where(hit, route_weight_ref[:, choice : choice + 1], weights)
    picked = picked.astype(jnp.bfloat16)
    weights_high = weights.astype(jnp.bfloat16)
    weights_low = (weights - weights_high.astype(jnp.float32)).astype(jnp.bfloat16)

    for copy in row_copies:
        copy.wait_recv()
    for source in range(tp_count):
        heads_ref[:, source * width : (source + 1) * width] = land_ref[source]
    proj_fetch.wait()
    stream_fetch.wait()
    square = jnp.zeros((tokens, 1), jnp.float32)
    for at in range(0, model, 512):
        part = dot_nn(heads_ref[...], proj_ref[:, at : at + 512])
        wide_ref[:, at : at + 512] = part
        square = square + jnp.sum(part * part, axis=-1, keepdims=True)
    scale = lax.rsqrt(square * (1.0 / model) + EPS)
    square = jnp.zeros((tokens, 1), jnp.float32)
    for at in range(0, model, 512):
        part = (
            stream_ref[:, at : at + 512].astype(jnp.float32)
            + wide_ref[:, at : at + 512] * scale * mix_gain_ref[:, at : at + 512]
        ).astype(jnp.bfloat16)
        residual_ref[:, at : at + 512] = part
        part = part.astype(jnp.float32)
        square = square + jnp.sum(part * part, axis=-1, keepdims=True)
    scale = lax.rsqrt(square * (1.0 / model) + EPS)
    for at in range(0, model, 512):
        part = (
            residual_ref[:, at : at + 512].astype(jnp.float32)
            * scale
            * ffn_gain_ref[:, at : at + 512]
        ).astype(jnp.bfloat16)
        normed_ref[:, at : at + 512] = part
        outgoing_ref[:, :, at : at + 512] = (
            dot_tn(picked, part).astype(jnp.bfloat16).reshape(sp_count, capacity, 512)
        )

    block_copies = [
        send(
            outgoing_ref.at[lax.rem(sp_me + step, sp_count)],
            arrived_ref.at[sp_me],
            block_send.at[step],
            block_recv.at[step],
            sp_peer(step),
        )
        for step in range(1, sp_count)
    ]
    arrived_ref[sp_me] = outgoing_ref[sp_me]

    for index in range(WEIGHT_EARLY):
        relay(index)
    for copy in spreads:
        copy.wait_recv()
    sides = []
    side = sp_me + 1 - 2 * lax.rem(sp_me, 2)
    for hop in range(team // 2):
        which = lax.rem(place + 2 * hop, team)
        for step in range(1, ranks):
            owner = lax.rem(rank + ranks - step, ranks) * 2 + seat
            for kind in range(3):
                sides.append(
                    send(
                        shared_slot(kind, owner, which),
                        shared_slot(kind, owner, which),
                        side_send.at[hop, step, kind],
                        side_recv.at[hop, step, kind],
                        (side, tp_me),
                    )
                )
    relay(WEIGHT_EARLY)
    relay(WEIGHT_EARLY + 1)
    for copy in sides:
        copy.wait_recv()
    lasts = []
    for step in range(1, ranks):
        owner = lax.rem(rank + ranks - step, ranks) * 2 + seat
        for kind in range(3):
            lasts.append(
                send(
                    shared_slot(kind, owner),
                    shared_slot(kind, owner),
                    last_send.at[step, kind],
                    last_recv.at[step, kind],
                    buddy,
                )
            )
    relay(WEIGHT_EARLY + 2)
    for copy in shared_fetches:
        copy.wait()
    for copy in near + lasts:
        copy.wait_recv()
    shared_hidden = jax.nn.silu(dot_nn(normed_ref[...], sgate_ref[...])) * dot_nn(
        normed_ref[...], sup_ref[...]
    )
    shared_hidden = shared_hidden.astype(jnp.bfloat16)
    for at in range(0, model, 512):
        wide_ref[:, at : at + 512] = dot_nn(shared_hidden, sdown_ref[:, at : at + 512])

    relay(WEIGHT_EARLY + 3)
    for index in range(2 * WEIGHT_CUTS):
        weight_fetches[index].wait()
        pairs[index].wait_recv()
        for copy in relays[index]:
            copy.wait_recv()
    relay(2 * WEIGHT_CUTS)
    for copy in block_copies:
        copy.wait_recv()
    rows_in = arrived_ref[...].reshape(slots, model)
    for owner in range(tp_count):
        hidden_ref[:, owner * part_width : (owner + 1) * part_width] = (
            jax.nn.silu(dot_nn(rows_in, gate_ref[owner])) * dot_nn(rows_in, up_ref[owner])
        ).astype(jnp.bfloat16)

    returns = []
    per_cut = WEIGHT_CUTS // return_cuts
    for part in range(return_cuts):
        for at in range(part * per_cut, (part + 1) * per_cut):
            index = 2 * WEIGHT_CUTS + at
            if at > 0:
                relay(index)
            weight_fetches[index].wait()
            pairs[index].wait_recv()
            for copy in relays[index]:
                copy.wait_recv()
            inner = pl.ds((at - part * per_cut) * piece, piece)
            done_ref[part, :, :, inner] = (
                dot_nn(hidden_ref[...], down_ref[at])
                .astype(jnp.bfloat16)
                .reshape(sp_count, capacity, piece)
            )
        returns.append(
            [
                send(
                    done_ref.at[part, lax.rem(sp_me + step, sp_count)],
                    back_ref.at[part, sp_me],
                    back_send.at[part, step],
                    back_recv.at[part, step],
                    sp_peer(step),
                )
                for step in range(1, sp_count)
            ]
        )
        back_ref[part, sp_me] = done_ref[part, sp_me]

    square = jnp.zeros((tokens, 1), jnp.float32)
    for part in range(return_cuts):
        for copy in returns[part]:
            copy.wait_recv()
        back = back_ref[part].reshape(slots, cut)
        inner = pl.ds(part * cut, cut)
        mixture = wide_ref[:, inner] + dot_nn(weights_high, back) + dot_nn(weights_low, back)
        wide_ref[:, inner] = mixture
        square = square + jnp.sum(mixture * mixture, axis=-1, keepdims=True)
    scale = lax.rsqrt(square * (1.0 / model) + EPS)
    for at in range(0, model, 512):
        out_ref[:, at : at + 512] = (
            residual_ref[:, at : at + 512].astype(jnp.float32)
            + wide_ref[:, at : at + 512] * scale * moe_gain_ref[:, at : at + 512]
        ).astype(out_ref.dtype)
    for copy in sends:
        copy.wait_send()


def body(
    stream,
    queries,
    key_rows,
    values,
    out_gate,
    fwd_decay,
    bwd_decay,
    head_gain,
    out_proj,
    mix_gain,
    ffn_gain,
    moe_gain,
    routes,
    route_weight,
    expert_gate,
    expert_up,
    expert_down,
    shared_gate,
    shared_up,
    shared_down,
):
    sp_count = lax.axis_size("sp")
    tp_count = lax.axis_size("tp")
    tokens, model = stream.shape
    span, lanes = queries.shape
    width = values.shape[1]
    blocks = span // BLK
    part_width = expert_gate.shape[2]
    shared_width = shared_gate.shape[1] * tp_count
    capacity = max(2, 3 * tokens * TOPK // (2 * sp_count))
    capacity = -(-capacity // ROW_TILE) * ROW_TILE
    slots = sp_count * capacity
    return_cuts = WEIGHT_CUTS if sp_count <= 16 else 1
    team = min(8, sp_count)
    ranks = tp_count // 2

    half = KEY_CHANNELS // 2
    lane = jnp.arange(lanes, dtype=jnp.int32) % KEY_CHANNELS
    frequency = ROPE_BASE ** (-(lane % half).astype(jnp.float32) / half)
    offset = lax.axis_index("sp") * span
    index = jnp.arange(BLK + blocks, dtype=jnp.int32)
    positions = jnp.where(index < BLK, index, offset + (index - BLK) * BLK).astype(jnp.float32)
    angles = positions[:, None] * frequency[None, :]
    sine = jnp.sin(angles)
    table = jnp.stack([jnp.cos(angles), jnp.where(lane[None, :] < half, -sine, sine)])

    vmem = pl.BlockSpec(memory_space=pltpu.VMEM)
    hbm = pl.BlockSpec(memory_space=pl.ANY)
    dma = pltpu.SemaphoreType.DMA
    bf16, f32 = jnp.bfloat16, jnp.float32
    count = 3 * WEIGHT_CUTS
    return pl.pallas_call(
        functools.partial(layer_kernel, sp_count, tp_count, capacity, return_cuts),
        out_shape=jax.ShapeDtypeStruct(stream.shape, stream.dtype),
        in_specs=[vmem] * 12 + [hbm] * 9,
        out_specs=vmem,
        scratch_shapes=[
            pltpu.VMEM(out_gate.shape, bf16),
            pltpu.VMEM(stream.shape, bf16),
            pltpu.VMEM(out_proj.shape, bf16),
            pltpu.VMEM((tp_count, model, part_width), bf16),
            pltpu.VMEM((tp_count, model, part_width), bf16),
            pltpu.VMEM((WEIGHT_CUTS, tp_count * part_width, model // WEIGHT_CUTS), bf16),
            pltpu.VMEM((model, shared_width), bf16),
            pltpu.VMEM((model, shared_width), bf16),
            pltpu.VMEM((shared_width, model), bf16),
            pltpu.VMEM((2, DV + 16, lanes), bf16),
            pltpu.VMEM((sp_count, DV + 16, lanes), bf16),
            pltpu.VMEM((span, width), bf16),
            pltpu.VMEM((tp_count, tokens, width), bf16),
            pltpu.VMEM((span, width), f32),
            pltpu.VMEM((span, lanes), f32),
            pltpu.VMEM((blocks, width, lanes), f32),
            pltpu.VMEM((blocks, width, lanes), f32),
            pltpu.VMEM((tokens, tp_count * width), bf16),
            pltpu.VMEM((tokens, model), f32),
            pltpu.VMEM((tokens, model), bf16),
            pltpu.VMEM((tokens, model), bf16),
            pltpu.VMEM((sp_count, capacity, model), bf16),
            pltpu.VMEM((sp_count, capacity, model), bf16),
            pltpu.VMEM((slots, tp_count * part_width), bf16),
            pltpu.VMEM((return_cuts, sp_count, capacity, model // return_cuts), bf16),
            pltpu.VMEM((return_cuts, sp_count, capacity, model // return_cuts), bf16),
            dma((6,)),
            dma((sp_count,)),
            dma((sp_count,)),
            dma((tp_count,)),
            dma((tp_count,)),
            dma((sp_count,)),
            dma((sp_count,)),
            dma((return_cuts, sp_count)),
            dma((return_cuts, sp_count)),
            dma((count,)),
            dma((count,)),
            dma((count,)),
            dma((ranks, count)),
            dma((ranks, count)),
            dma((ranks, count)),
            dma((ranks, count)),
            dma((3,)),
            dma((3,)),
            dma((ranks, 3)),
            dma((ranks, 3)),
            dma((team // 2, ranks, 3)),
            dma((team // 2, ranks, 3)),
            dma((team // 2, ranks, 3)),
            dma((team // 2, ranks, 3)),
            dma((ranks, 3)),
            dma((ranks, 3)),
        ],
        compiler_params=pltpu.CompilerParams(
            collective_id=0, has_side_effects=True, vmem_limit_bytes=62 * 2**20
        ),
    )(
        queries,
        key_rows,
        values,
        fwd_decay,
        bwd_decay,
        table,
        head_gain.reshape(1, -1),
        mix_gain.reshape(1, -1),
        ffn_gain.reshape(1, -1),
        moe_gain.reshape(1, -1),
        routes,
        route_weight,
        out_gate,
        stream,
        out_proj,
        expert_gate,
        expert_up,
        expert_down,
        shared_gate,
        shared_up,
        shared_down,
    )


def solution(mesh):
    return jax.shard_map(
        body,
        mesh=mesh,
        in_specs=(
            P(("sp", "tp"), None),
            P("sp", "tp"),
            P("sp", "tp"),
            P("sp", "tp"),
            P("sp", "tp"),
            P("sp", "tp"),
            P("sp", "tp"),
            P("tp"),
            P(),
            P(),
            P(),
            P(),
            P(("sp", "tp"), None),
            P(("sp", "tp"), None),
            P("sp", None, "tp"),
            P("sp", None, "tp"),
            P("sp", "tp", None),
            P(None, "tp"),
            P(None, "tp"),
            P("tp", None),
        ),
        out_specs=P(("sp", "tp"), None),
        check_vma=False,
    )
```

```python
import functools

import jax
import jax.numpy as jnp
import numpy as np
from jax import lax
from jax.experimental import pallas as pl
from jax.experimental.pallas import tpu as pltpu
from jax.sharding import PartitionSpec as P

KEY_CHANNELS = 64
DV = 128
BLK = 64
TOPK = 2
ROW_TILE = 16


EPS = 1e-06
GATE_NORM = 16.0
ROPE_BASE = 10000.0
MESH = pl.DeviceIdType.MESH
DEPTH_CUTS = 4
DOWN_CUTS = 8
PIECES_EARLY = 1


def dot_nn(left, right):
    return jnp.dot(left, right, preferred_element_type=jnp.float32)


def dot_nt(left, right):
    return lax.dot_general(
        left, right, (((1,), (1,)), ((), ())), preferred_element_type=jnp.float32
    )


def dot_tn(left, right):
    return lax.dot_general(
        left, right, (((0,), (0,)), ((), ())), preferred_element_type=jnp.float32
    )


def layer_kernel(
    sp_count,
    tp_count,
    capacity,
    return_cuts,
    fwd_hbm,
    bwd_hbm,
    k_hbm,
    v_hbm,
    table_hbm,
    q_hbm,
    out_gate_hbm,
    gain_hbm,
    stream_hbm,
    routes_hbm,
    route_weight_hbm,
    mix_gain_hbm,
    ffn_gain_hbm,
    moe_gain_hbm,
    proj_hbm,
    gate_hbm,
    up_hbm,
    down_hbm,
    shared_gate_hbm,
    shared_up_hbm,
    shared_down_hbm,
    out_ref,
    fwd_ref,
    bwd_ref,
    k_ref,
    v_ref,
    table_ref,
    q_ref,
    out_gate_ref,
    gain_ref,
    stream_ref,
    routes_ref,
    route_weight_ref,
    mix_gain_ref,
    ffn_gain_ref,
    moe_gain_ref,
    proj_ref,
    gate_ref,
    up_ref,
    down_ref,
    sgate_ref,
    sup_ref,
    sdown_ref,
    own_ref,
    got_ref,
    mixed_ref,
    land_ref,
    within_ref,
    key_ref,
    sums_f,
    sums_b,
    heads_ref,
    wide_ref,
    residual_ref,
    normed_ref,
    outgoing_ref,
    arrived_ref,
    silu_ref,
    hidden_ref,
    done_ref,
    back_ref,
    local_sem,
    sum_send,
    sum_recv,
    row_send,
    row_recv,
    block_send,
    block_recv,
    back_send,
    back_recv,
    weight_sem,
    pair_send,
    pair_recv,
    cross_send,
    cross_recv,
    relay_send,
    relay_recv,
    near_send,
    near_recv,
    slice_send,
    slice_recv,
    spread_send,
    spread_recv,
    last_send,
    last_recv,
):
    span, lanes = q_ref.shape
    width = v_ref.shape[1]
    heads = lanes // KEY_CHANNELS
    blocks = span // BLK
    tokens = span // tp_count
    model = stream_ref.shape[1]
    part_width = gate_hbm.shape[2]
    slots = sp_count * capacity
    cut = model // return_cuts
    depth = model // DEPTH_CUTS
    piece = model // DOWN_CUTS
    sp_me = lax.axis_index("sp")
    tp_me = lax.axis_index("tp")
    ranks = tp_count // 2
    rank = lax.div(tp_me, 2)
    seat = lax.rem(tp_me, 2)
    buddy = (sp_me, tp_me + 1 - 2 * seat)
    team = min(8, sp_count)
    place = lax.rem(sp_me, team)
    team_base = sp_me - place
    drains = []

    def sp_peer(step):
        return (lax.rem(sp_me + step, sp_count), tp_me)

    def tp_peer(step):
        return (sp_me, lax.rem(tp_me + step, tp_count))

    def flip(index, mask):
        result, bit = index, 1
        while bit <= mask:
            if mask & bit:
                result = result + bit * (1 - 2 * lax.rem(lax.div(index, bit), 2))
            bit = 2 * bit
        return result

    def mate(distance):
        return (flip(sp_me, distance), tp_me)

    def cross_tp(step):
        return lax.rem(rank + step, ranks) * 2 + seat

    def remote(source, target, send_sem, recv_sem, device):
        return pltpu.make_async_remote_copy(
            src_ref=source,
            dst_ref=target,
            send_sem=send_sem,
            recv_sem=recv_sem,
            device_id=device,
            device_id_type=MESH,
        )

    def send(source, target, send_sem, recv_sem, device):
        copy = remote(source, target, send_sem, recv_sem, device)
        copy.start()
        return copy

    def wait_bytes(ref, semaphore):
        remote(ref, ref, semaphore, semaphore, buddy).wait_recv()

    def sent_bytes(ref, semaphore):
        drains.append(remote(ref, ref, semaphore, semaphore, buddy))

    def fetch(source, target, semaphore):
        copy = pltpu.make_async_copy(source, target, semaphore)
        copy.start()
        return copy

    barrier = pltpu.get_barrier_semaphore()
    for step in range(1, sp_count):
        pl.semaphore_signal(barrier, inc=1, device_id=sp_peer(step), device_id_type=MESH)
    for step in range(1, tp_count):
        pl.semaphore_signal(barrier, inc=1, device_id=tp_peer(step), device_id_type=MESH)
    inputs = [
        fetch(source, target, local_sem.at[at])
        for at, (source, target) in enumerate(
            (
                (fwd_hbm, fwd_ref),
                (bwd_hbm, bwd_ref),
                (k_hbm, k_ref),
                (v_hbm, v_ref),
                (table_hbm, table_ref),
                (q_hbm, q_ref),
                (out_gate_hbm, out_gate_ref),
                (gain_hbm, gain_ref),
                (stream_hbm, stream_ref),
                (routes_hbm, routes_ref),
                (route_weight_hbm, route_weight_ref),
                (mix_gain_hbm, mix_gain_ref),
                (ffn_gain_hbm, ffn_gain_ref),
                (moe_gain_hbm, moe_gain_ref),
            )
        )
    ]

    pieces = [(kind, at) for kind in range(2) for at in range(DEPTH_CUTS)]
    first_down = len(pieces)
    pieces = pieces + [(2, at) for at in range(DOWN_CUTS)]
    count = len(pieces)
    groups = [(0, 0), (1, 0)] + [(2, at) for at in range(DOWN_CUTS)]

    def group_of(index):
        kind, at = pieces[index]
        return 2 + at if kind == 2 else kind

    def group_source(group):
        kind, at = groups[group]
        if kind < 2:
            return (gate_hbm, up_hbm)[kind].at[0]
        return down_hbm.at[0, :, pl.ds(at * piece, piece)]

    def group_slot(group, owner):
        kind, at = groups[group]
        if kind < 2:
            return (gate_ref, up_ref)[kind].at[owner]
        row = pl.multiple_of(owner * part_width, part_width)
        return down_ref.at[at, pl.ds(row, part_width), :]

    def weight_slot(index, owner):
        kind, at = pieces[index]
        if kind < 2:
            return (gate_ref, up_ref)[kind].at[owner, pl.ds(at * depth, depth), :]
        return group_slot(group_of(index), owner)

    shared_lanes = shared_gate_hbm.shape[1]

    def shared_slot(kind, owner, which=None):
        if kind < 2:
            ref = (sgate_ref, sup_ref)[kind].at[owner]
            size = model // team
        else:
            row = pl.multiple_of(owner * shared_lanes, shared_lanes)
            ref = sdown_ref.at[pl.ds(row, shared_lanes), :]
            size = shared_lanes // team
        if which is None:
            return ref
        return ref.at[pl.ds(pl.multiple_of(which * size, size), size), :]

    def shared_source(kind, which=None):
        ref = (shared_gate_hbm, shared_up_hbm, shared_down_hbm)[kind]
        if which is None:
            return ref
        size = (shared_lanes if kind == 2 else model) // team
        return ref.at[pl.ds(pl.multiple_of(which * size, size), size), :]

    shared_fetches = [
        fetch(shared_source(kind), shared_slot(kind, tp_me), local_sem.at[len(inputs) + kind])
        for kind in range(3)
    ]
    weight_fetches = [
        fetch(group_source(group), group_slot(group, tp_me), weight_sem.at[group])
        for group in range(len(groups))
    ]

    inputs.append(fetch(proj_hbm, proj_ref, local_sem.at[len(inputs) + 3]))

    row = lax.broadcasted_iota(jnp.int32, (BLK, BLK), 0)
    column = lax.broadcasted_iota(jnp.int32, (BLK, BLK), 1)
    lower = row >= column
    upper = row <= column
    lower_ones = lower.astype(jnp.bfloat16)
    upper_ones = upper.astype(jnp.bfloat16)
    from_lane = lax.broadcasted_iota(jnp.int32, (lanes, lanes), 0)
    to_lane = lax.broadcasted_iota(jnp.int32, (lanes, lanes), 1)
    half = KEY_CHANNELS // 2
    partner = jnp.where(lax.rem(to_lane, KEY_CHANNELS) < half, to_lane + half, to_lane - half)
    swap = (from_lane == partner).astype(jnp.bfloat16)
    own_head = (
        lax.broadcasted_iota(jnp.int32, (width, lanes), 0) // DV
        == lax.broadcasted_iota(jnp.int32, (width, lanes), 1) // KEY_CHANNELS
    )
    lane_head = lax.broadcasted_iota(jnp.int32, (BLK, lanes), 1) // KEY_CHANNELS

    def rotated(tensor, block):
        at = pl.ds(BLK + sp_me * blocks + block, 1)
        cos_at, sin_at = table_ref[0, at, :], table_ref[1, at, :]
        cos_row, sin_row = table_ref[0, 0:BLK, :], table_ref[1, 0:BLK, :]
        cosine = cos_row * cos_at - sin_row * sin_at
        sine = sin_row * cos_at + cos_row * sin_at
        return tensor.astype(jnp.float32) * cosine + dot_nn(tensor, swap) * sine

    def running(ones, raw):
        logs = (jnp.minimum(raw, 0.0) - jnp.log1p(jnp.exp(-jnp.abs(raw)))) * (1.0 / GATE_NORM)
        first = logs.astype(jnp.bfloat16)
        rest = logs - first.astype(jnp.float32)
        second = rest.astype(jnp.bfloat16)
        third = (rest - second.astype(jnp.float32)).astype(jnp.bfloat16)
        return dot_nn(ones, first) + (dot_nn(ones, second) + dot_nn(ones, third))

    pl.semaphore_wait(barrier, sp_count - 1 + tp_count - 1)

    near, slices = [], []
    for kind in range(3):
        for step in range(1, ranks):
            slices.append(
                send(
                    shared_source(kind, place),
                    shared_slot(kind, tp_me, place),
                    slice_send.at[step - 1, kind],
                    slice_recv.at[step - 1, kind],
                    (sp_me, cross_tp(step)),
                )
            )

    crossings = {}
    whole = (gate_hbm.at[0], up_hbm.at[0], down_hbm.at[0])

    fetched = set()

    def cross(index):
        kind, group = pieces[index][0], group_of(index)
        if group not in fetched:
            fetched.add(group)
            weight_fetches[group].wait()
        crossings[index] = [
            send(
                weight_slot(index, tp_me),
                weight_slot(index, tp_me),
                cross_send.at[step - 1, kind],
                cross_recv.at[step - 1, index],
                (sp_me, cross_tp(step)),
            )
            for step in range(1, ranks)
        ]

    def relay(index):
        kind = pieces[index][0]
        for step in range(1, ranks):
            crossings[index][step - 1].wait_recv()
            owner = lax.rem(rank + ranks - step, ranks) * 2 + seat
            send(
                weight_slot(index, owner),
                weight_slot(index, owner),
                relay_send.at[step - 1, kind],
                relay_recv.at[step - 1, group_of(index)],
                buddy,
            )

    for kind in range(3):
        sent_bytes(whole[kind], pair_send.at[kind])
        for step in range(1, ranks):
            sent_bytes(whole[kind], cross_send.at[step - 1, kind])
            sent_bytes(whole[kind], relay_send.at[step - 1, kind])

    for index in range(PIECES_EARLY):
        cross(index)
    for kind in range(3):
        near.append(
            send(
                shared_source(kind),
                shared_slot(kind, tp_me),
                near_send.at[kind],
                near_recv.at[kind],
                buddy,
            )
        )
    pairs = [
        send(
            group_slot(group, tp_me) if group in fetched else group_source(group),
            group_slot(group, tp_me),
            pair_send.at[groups[group][0]],
            pair_recv.at[group],
            buddy,
        )
        for group in range(len(groups))
    ]

    for copy in inputs[:5]:
        copy.wait()
    cumul_f, cumul_b, decay_f, decay_b = [], [], [], []
    for block in range(blocks):
        rows = pl.ds(block * BLK, BLK)
        total_f = running(lower_ones, fwd_ref[rows, :])
        total_b = running(upper_ones, bwd_ref[rows, :])
        last_f = total_f[BLK - 1 : BLK]
        last_b = total_b[0:1]
        keys = rotated(k_ref[rows, :], block)
        key_ref[rows, :] = keys
        value_rows = v_ref[rows, :]
        out_f = (keys * jnp.exp(last_f - total_f)).astype(jnp.bfloat16)
        out_b = (keys * jnp.exp(last_b - total_b)).astype(jnp.bfloat16)
        sums_f[block] = jnp.where(own_head, dot_tn(value_rows, out_f), 0.0)
        sums_b[block] = jnp.where(own_head, dot_tn(value_rows, out_b), 0.0)
        cumul_f.append(total_f)
        cumul_b.append(total_b)
        decay_f.append(jnp.exp(last_f))
        decay_b.append(jnp.exp(last_b))

    def packed(total):
        return sum(total[h * DV : (h + 1) * DV] for h in range(heads))

    total = sums_f[0]
    through = decay_f[0]
    for block in range(1, blocks):
        total = total * decay_f[block] + sums_f[block]
        through = through * decay_f[block]
    own_ref[0, 0:DV, :] = packed(total).astype(jnp.bfloat16)
    own_ref[0, DV : DV + 16, :] = jnp.broadcast_to(through, (16, lanes)).astype(jnp.bfloat16)
    total = sums_b[blocks - 1]
    through = decay_b[blocks - 1]
    for block in range(blocks - 2, -1, -1):
        total = total * decay_b[block] + sums_b[block]
        through = through * decay_b[block]
    own_ref[1, 0:DV, :] = packed(total).astype(jnp.bfloat16)
    own_ref[1, DV : DV + 16, :] = jnp.broadcast_to(through, (16, lanes)).astype(jnp.bfloat16)

    for step in range(1, sp_count):
        send(
            own_ref.at[lax.div(sp_me + step, sp_count)],
            got_ref.at[step],
            sum_send.at[0],
            sum_recv.at[0],
            sp_peer(step),
        )
    others = pl.ds(1, sp_count - 1)
    sent_bytes(got_ref.at[others], sum_send.at[0])
    inputs[5].wait()
    query_f, query_b = [], []
    for block in range(blocks):
        rows = pl.ds(block * BLK, BLK)
        queries = rotated(q_ref[rows, :], block) * KEY_CHANNELS ** (-0.5)
        keys = key_ref[rows, :]
        total_f, total_b = cumul_f[block], cumul_b[block]
        middle_f = total_f[BLK // 2 - 1 : BLK // 2]
        middle_b = total_b[BLK // 2 : BLK // 2 + 1]
        scaled_qf = queries * jnp.exp(total_f - middle_f)
        scaled_qb = queries * jnp.exp(total_b - middle_b)
        scaled_kf = (keys * jnp.exp(middle_f - total_f)).astype(jnp.bfloat16)
        scaled_kb = (keys * jnp.exp(middle_b - total_b)).astype(jnp.bfloat16)
        query_f.append((queries * jnp.exp(total_f)).astype(jnp.bfloat16))
        query_b.append((queries * jnp.exp(total_b)).astype(jnp.bfloat16))
        for h in range(heads):
            mine = lane_head == h
            scores_f = dot_nt(jnp.where(mine, scaled_qf, 0.0).astype(jnp.bfloat16), scaled_kf)
            scores_b = dot_nt(jnp.where(mine, scaled_qb, 0.0).astype(jnp.bfloat16), scaled_kb)
            scores = jnp.where(lower, scores_f, 0.0) + jnp.where(upper, scores_b, 0.0)
            within_ref[rows, h * DV : (h + 1) * DV] = dot_nn(
                scores.astype(jnp.bfloat16), v_ref[rows, h * DV : (h + 1) * DV]
            )
    wait_bytes(got_ref.at[others], sum_recv.at[0])
    carry_f = jnp.zeros((DV, lanes), jnp.float32)
    carry_b = jnp.zeros((DV, lanes), jnp.float32)
    for step in range(sp_count - 1, 0, -1):
        state = got_ref[step, 0:DV, :].astype(jnp.float32)
        through = got_ref[step, DV : DV + 16, :].astype(jnp.float32)[0:1]
        carry_f = jnp.where(step <= sp_me, carry_f * through + state, carry_f)
    for step in range(1, sp_count):
        state = got_ref[step, 0:DV, :].astype(jnp.float32)
        through = got_ref[step, DV : DV + 16, :].astype(jnp.float32)[0:1]
        carry_b = jnp.where(step > sp_me, carry_b * through + state, carry_b)

    def unpacked(carry):
        return jnp.where(own_head, jnp.concatenate([carry] * heads, axis=0), 0.0)

    state = unpacked(carry_f)
    for block in range(blocks):
        rows = pl.ds(block * BLK, BLK)
        within_ref[rows, :] += dot_nt(query_f[block], state.astype(jnp.bfloat16))
        if block < blocks - 1:
            state = state * decay_f[block] + sums_f[block]
    inputs[6].wait()
    inputs[7].wait()
    state = unpacked(carry_b)
    for block in range(blocks - 1, -1, -1):
        rows = pl.ds(block * BLK, BLK)
        attended = within_ref[rows, :] + dot_nt(query_b[block], state.astype(jnp.bfloat16))
        if block > 0:
            state = state * decay_b[block] + sums_b[block]
        for h in range(heads):
            part = attended[:, h * DV : (h + 1) * DV]
            square = jnp.mean(part * part, axis=-1, keepdims=True)
            gate = out_gate_ref[rows, h * DV : (h + 1) * DV].astype(jnp.float32)
            mixed_ref[rows, h * DV : (h + 1) * DV] = (
                part
                * lax.rsqrt(square + EPS)
                * gain_ref[:, h * DV : (h + 1) * DV]
                * (gate / (1.0 + jnp.exp(-gate)))
            ).astype(jnp.bfloat16)

    row_copies = []
    for step in range(1, tp_count):
        target = lax.rem(tp_me + step, tp_count)
        row_copies.append(
            send(
                mixed_ref.at[pl.ds(pl.multiple_of(target * tokens, tokens), tokens)],
                land_ref.at[tp_me],
                row_send.at[0],
                row_recv.at[step],
                (sp_me, target),
            )
        )
    sent_bytes(mixed_ref.at[pl.ds(0, (tp_count - 1) * tokens)], row_send.at[0])
    for index in range(PIECES_EARLY, count):
        cross(index)
    spread_masks = [0]
    spread_copies = slices
    spread_count = 0

    def spread(bit):
        nonlocal spread_masks, spread_copies, spread_count
        for copy in spread_copies:
            copy.wait_recv()
        spread_copies = []
        for mask in spread_masks:
            which = flip(place, mask)
            for step in range(1, ranks):
                owner = lax.rem(rank + ranks - step, ranks) * 2 + seat
                for kind in range(3):
                    spread_copies.append(
                        send(
                            shared_slot(kind, owner, which),
                            shared_slot(kind, owner, which),
                            spread_send.at[step - 1, kind],
                            spread_recv.at[step - 1, spread_count, kind],
                            mate(bit),
                        )
                    )
            spread_count += 1
        spread_masks = spread_masks + [mask + bit for mask in spread_masks]

    stages = [team >> shift for shift in range(1, team.bit_length())]
    spread(stages[0])
    land_ref[tp_me] = mixed_ref[pl.ds(pl.multiple_of(tp_me * tokens, tokens), tokens), :]

    for copy in inputs[8:]:
        copy.wait()
    token_row = lax.broadcasted_iota(jnp.int32, (tokens, tokens), 0)
    token_column = lax.broadcasted_iota(jnp.int32, (tokens, tokens), 1)
    earlier = (token_row < token_column).astype(jnp.bfloat16)
    expert_row = lax.broadcasted_iota(jnp.int32, (max(8, sp_count), tokens), 0)
    choices = [routes_ref[choice : choice + 1, :] for choice in range(TOPK)]
    named = [(chosen == expert_row).astype(jnp.float32) for chosen in choices]
    before = dot_nn(sum(named).astype(jnp.bfloat16), earlier)
    slot_row = lax.broadcasted_iota(jnp.int32, (slots, tokens), 0)
    weights = jnp.zeros((slots, tokens), jnp.float32)
    picked = jnp.zeros((slots, tokens), jnp.float32)
    for choice in range(TOPK):
        slot = jnp.sum(before * named[choice], axis=0, keepdims=True).astype(jnp.int32)
        distance = lax.bitwise_xor(choices[choice], jnp.full((1, tokens), sp_me, jnp.int32))
        hit = slot_row == distance * capacity + slot
        picked = jnp.where(hit, 1.0, picked)
        weights = jnp.where(hit, route_weight_ref[choice : choice + 1, :], weights)
    picked = picked.astype(jnp.bfloat16)
    weights = jnp.transpose(weights)
    weights_high = weights.astype(jnp.bfloat16)
    weights_low = (weights - weights_high.astype(jnp.float32)).astype(jnp.bfloat16)

    for copy in row_copies:
        copy.wait_recv()
    for source in range(tp_count):
        heads_ref[:, source * width : (source + 1) * width] = land_ref[source]
    square = jnp.zeros((tokens, 1), jnp.float32)
    for at in range(0, model, 512):
        part = dot_nn(heads_ref[...], proj_ref[:, at : at + 512])
        wide_ref[:, at : at + 512] = part
        square = square + jnp.sum(part * part, axis=-1, keepdims=True)
    scale = lax.rsqrt(square * (1.0 / model) + EPS)
    square = jnp.zeros((tokens, 1), jnp.float32)
    for at in range(0, model, 512):
        part = (
            stream_ref[:, at : at + 512].astype(jnp.float32)
            + wide_ref[:, at : at + 512] * scale * mix_gain_ref[:, at : at + 512]
        ).astype(jnp.bfloat16)
        residual_ref[:, at : at + 512] = part
        part = part.astype(jnp.float32)
        square = square + jnp.sum(part * part, axis=-1, keepdims=True)
    scale = lax.rsqrt(square * (1.0 / model) + EPS)
    for at in range(0, model, 512):
        part = (
            residual_ref[:, at : at + 512].astype(jnp.float32)
            * scale
            * ffn_gain_ref[:, at : at + 512]
        ).astype(jnp.bfloat16)
        normed_ref[:, at : at + 512] = part
        outgoing_ref[:, :, at : at + 512] = (
            dot_nn(picked, part).astype(jnp.bfloat16).reshape(sp_count, capacity, 512)
        )

    far = sp_count // 2
    order = list(range(far, sp_count)) + list(range(1, far))
    for distance in order:
        send(
            outgoing_ref.at[distance],
            arrived_ref.at[distance],
            block_send.at[0],
            block_recv.at[distance // far],
            mate(distance),
        )
    sent_bytes(outgoing_ref.at[others], block_send.at[0])
    for bit in stages[1:-1]:
        spread(bit)
    arrived_ref[0] = outgoing_ref[0]

    for index in range(PIECES_EARLY):
        relay(index)

    def arrive(group):
        pairs[group].wait_recv()
        for step in range(1, ranks):
            owner = lax.rem(rank + ranks - step, ranks) * 2 + 1 - seat
            wait_bytes(group_slot(group, owner), relay_recv.at[step - 1, group])

    def put_hidden(owner, low, high, values):
        lane = owner * part_width
        hidden_ref[low * capacity : high * capacity, lane : lane + part_width] = values.astype(
            jnp.bfloat16
        )

    middle = first_down // 2
    for index in range(PIECES_EARLY, middle):
        relay(index)
    if len(stages) > 1:
        spread(stages[-1])
    for index in range(middle, first_down - 2):
        relay(index)
    arrive(0)

    def wait_blocks(low, high):
        inner = pl.ds(max(low, 1), high - max(low, 1))
        if high > max(low, 1):
            wait_bytes(arrived_ref.at[inner], block_recv.at[low // far])

    def rows_of(low, high):
        return arrived_ref[low:high].reshape((high - low) * capacity, model)

    per_cut = DOWN_CUTS // return_cuts

    def give_back(part, low, high):
        for at in range(part * per_cut, (part + 1) * per_cut):
            inner = pl.ds((at - part * per_cut) * piece, piece)
            done_ref[part, low:high, :, inner] = (
                dot_nn(hidden_ref[low * capacity : high * capacity, :], down_ref[at])
                .astype(jnp.bfloat16)
                .reshape(high - low, capacity, piece)
            )
        for distance in order:
            if low <= distance < high:
                send(
                    done_ref.at[part, distance],
                    back_ref.at[part, distance],
                    back_send.at[0],
                    back_recv.at[part],
                    mate(distance),
                )

    def down_ready(part):
        for at in range(part * per_cut, (part + 1) * per_cut):
            relay(first_down + at)
            arrive(2 + at)

    wait_blocks(far, sp_count)
    rows = rows_of(far, sp_count)
    for owner in range(tp_count):
        lane = owner * part_width
        silu_ref[:, lane : lane + part_width] = jax.nn.silu(dot_nn(rows, gate_ref[owner]))
    relay(first_down - 2)
    relay(first_down - 1)
    arrive(1)
    for owner in range(tp_count):
        lane = owner * part_width
        values = silu_ref[:, lane : lane + part_width] * dot_nn(rows, up_ref[owner])
        put_hidden(owner, far, sp_count, values)
    down_ready(0)
    give_back(0, far, sp_count)
    wait_blocks(0, far)
    rows = rows_of(0, far)
    for owner in range(tp_count):
        values = jax.nn.silu(dot_nn(rows, gate_ref[owner])) * dot_nn(rows, up_ref[owner])
        put_hidden(owner, 0, far, values)
    give_back(0, 0, far)
    for part in range(1, return_cuts):
        down_ready(part)
        give_back(part, 0, sp_count)
    for part in range(return_cuts):
        back_ref[part, 0] = done_ref[part, 0]
    sent_bytes(done_ref.at[:, others], back_send.at[0])

    for copy in spread_copies:
        copy.wait_recv()
    lasts = []
    for step in range(1, ranks):
        owner = lax.rem(rank + ranks - step, ranks) * 2 + seat
        for kind in range(3):
            lasts.append(
                send(
                    shared_slot(kind, owner),
                    shared_slot(kind, owner),
                    last_send.at[step - 1, kind],
                    last_recv.at[step - 1, kind],
                    buddy,
                )
            )
    for copy in shared_fetches:
        copy.wait()
    for copy in near + lasts:
        copy.wait_recv()
    shared_hidden = jnp.concatenate(
        [
            jax.nn.silu(dot_nn(normed_ref[...], sgate_ref[owner]))
            * dot_nn(normed_ref[...], sup_ref[owner])
            for owner in range(tp_count)
        ],
        axis=1,
    ).astype(jnp.bfloat16)
    for at in range(0, model, 512):
        wide_ref[:, at : at + 512] = dot_nn(shared_hidden, sdown_ref[:, at : at + 512])

    square = jnp.zeros((tokens, 1), jnp.float32)
    for part in range(return_cuts):
        wait_bytes(back_ref.at[part, others], back_recv.at[part])
        back = back_ref[part].reshape(slots, cut)
        inner = pl.ds(part * cut, cut)
        mixture = wide_ref[:, inner] + dot_nn(weights_high, back) + dot_nn(weights_low, back)
        wide_ref[:, inner] = mixture
        square = square + jnp.sum(mixture * mixture, axis=-1, keepdims=True)
    scale = lax.rsqrt(square * (1.0 / model) + EPS)
    for at in range(0, model, 512):
        out_ref[:, at : at + 512] = (
            residual_ref[:, at : at + 512].astype(jnp.float32)
            + wide_ref[:, at : at + 512] * scale * moe_gain_ref[:, at : at + 512]
        ).astype(out_ref.dtype)
    for kind in range(3):
        size = (shared_lanes if kind == 2 else model) // team * (team - 1)
        ref = (sgate_ref, sup_ref, sdown_ref)[kind]
        for step in range(1, ranks):
            if kind == 2:
                sent_bytes(ref.at[pl.ds(0, size), :], spread_send.at[step - 1, kind])
            else:
                sent_bytes(ref.at[0, pl.ds(0, size), :], spread_send.at[step - 1, kind])
    for copy in slices + near + lasts + drains:
        copy.wait_send()


def body(
    stream,
    queries,
    key_rows,
    values,
    out_gate,
    fwd_decay,
    bwd_decay,
    head_gain,
    out_proj,
    mix_gain,
    ffn_gain,
    moe_gain,
    routes,
    route_weight,
    expert_gate,
    expert_up,
    expert_down,
    shared_gate,
    shared_up,
    shared_down,
):
    sp_count = lax.axis_size("sp")
    tp_count = lax.axis_size("tp")
    tokens, model = stream.shape
    span, lanes = queries.shape
    width = values.shape[1]
    blocks = span // BLK
    part_width = expert_gate.shape[2]
    shared_width = shared_gate.shape[1] * tp_count
    capacity = max(2, 3 * tokens * TOPK // (2 * sp_count))
    capacity = -(-capacity // ROW_TILE) * ROW_TILE
    slots = sp_count * capacity
    return_cuts = DOWN_CUTS if sp_count <= 16 else 1
    team = min(8, sp_count)
    ranks = tp_count // 2

    half = KEY_CHANNELS // 2
    lane = np.arange(lanes) % KEY_CHANNELS
    frequency = ROPE_BASE ** (-(lane % half) / half)
    positions = np.concatenate([np.arange(BLK), np.arange(sp_count * blocks) * BLK])
    angles = positions[:, None] * frequency[None, :]
    sign = np.where(lane < half, -1.0, 1.0)
    table = jnp.asarray(np.stack([np.cos(angles), np.sin(angles) * sign]), jnp.float32)

    vmem = pl.BlockSpec(memory_space=pltpu.VMEM)
    hbm = pl.BlockSpec(memory_space=pl.ANY)
    dma = pltpu.SemaphoreType.DMA
    bf16, f32 = jnp.bfloat16, jnp.float32
    count = 2 * DEPTH_CUTS + DOWN_CUTS
    groups = 2 + DOWN_CUTS
    inputs = (
        fwd_decay,
        bwd_decay,
        key_rows,
        values,
        table,
        queries,
        out_gate,
        head_gain.reshape(1, -1),
        stream,
        routes.T,
        route_weight.T,
        mix_gain.reshape(1, -1),
        ffn_gain.reshape(1, -1),
        moe_gain.reshape(1, -1),
        out_proj,
    )
    updated = pl.pallas_call(
        functools.partial(layer_kernel, sp_count, tp_count, capacity, return_cuts),
        out_shape=jax.ShapeDtypeStruct(stream.shape, bf16),
        in_specs=[hbm] * (len(inputs) + 6),
        out_specs=vmem,
        scratch_shapes=[
            *(pltpu.VMEM(array.shape, array.dtype) for array in inputs),
            pltpu.VMEM((tp_count, model, part_width), bf16),
            pltpu.VMEM((tp_count, model, part_width), bf16),
            pltpu.VMEM((DOWN_CUTS, tp_count * part_width, model // DOWN_CUTS), bf16),
            pltpu.VMEM((tp_count, model, shared_width // tp_count), bf16),
            pltpu.VMEM((tp_count, model, shared_width // tp_count), bf16),
            pltpu.VMEM((shared_width, model), bf16),
            pltpu.VMEM((2, DV + 16, lanes), bf16),
            pltpu.VMEM((sp_count, DV + 16, lanes), bf16),
            pltpu.VMEM((span, width), bf16),
            pltpu.VMEM((tp_count, tokens, width), bf16),
            pltpu.VMEM((span, width), f32),
            pltpu.VMEM((span, lanes), f32),
            pltpu.VMEM((blocks, width, lanes), f32),
            pltpu.VMEM((blocks, width, lanes), f32),
            pltpu.VMEM((tokens, tp_count * width), bf16),
            pltpu.VMEM((tokens, model), f32),
            pltpu.VMEM((tokens, model), bf16),
            pltpu.VMEM((tokens, model), bf16),
            pltpu.VMEM((sp_count, capacity, model), bf16),
            pltpu.VMEM((sp_count, capacity, model), bf16),
            pltpu.VMEM((slots // 2, tp_count * part_width), f32),
            pltpu.VMEM((slots, tp_count * part_width), bf16),
            pltpu.VMEM((return_cuts, sp_count, capacity, model // return_cuts), bf16),
            pltpu.VMEM((return_cuts, sp_count, capacity, model // return_cuts), bf16),
            dma((len(inputs) + 3,)),
            dma((1,)),
            dma((1,)),
            dma((1,)),
            dma((tp_count,)),
            dma((1,)),
            dma((2,)),
            dma((1,)),
            dma((return_cuts,)),
            dma((groups,)),
            dma((3,)),
            dma((groups,)),
            dma((ranks - 1, 3)),
            dma((ranks - 1, count)),
            dma((ranks - 1, 3)),
            dma((ranks - 1, groups)),
            dma((3,)),
            dma((3,)),
            dma((ranks - 1, 3)),
            dma((ranks - 1, 3)),
            dma((ranks - 1, 3)),
            dma((ranks - 1, team - 1, 3)),
            dma((ranks - 1, 3)),
            dma((ranks - 1, 3)),
        ],
        compiler_params=pltpu.CompilerParams(
            collective_id=0, has_side_effects=True, vmem_limit_bytes=62 * 2**20
        ),
    )(
        *inputs,
        expert_gate,
        expert_up,
        expert_down,
        shared_gate,
        shared_up,
        shared_down,
    )
    return updated


def solution(mesh):
    return jax.shard_map(
        body,
        mesh=mesh,
        in_specs=(
            P(("sp", "tp"), None),
            P("sp", "tp"),
            P("sp", "tp"),
            P("sp", "tp"),
            P("sp", "tp"),
            P("sp", "tp"),
            P("sp", "tp"),
            P("tp"),
            P(),
            P(),
            P(),
            P(),
            P(("sp", "tp"), None),
            P(("sp", "tp"), None),
            P("sp", None, "tp"),
            P("sp", None, "tp"),
            P("sp", "tp", None),
            P(None, "tp"),
            P(None, "tp"),
            P("tp", None),
        ),
        out_specs=P(("sp", "tp"), None),
        check_vma=False,
    )
```

```python
import functools

import jax
import jax.numpy as jnp
import numpy as np
from jax import lax
from jax.experimental import pallas as pl
from jax.experimental.pallas import tpu as pltpu
from jax.sharding import PartitionSpec as P

KEY_CHANNELS = 64
DV = 128
BLK = 64
TOPK = 2
ROW_TILE = 16


EPS = 1e-06
GATE_NORM = 16.0
ROPE_BASE = 10000.0
MESH = pl.DeviceIdType.MESH
DEPTH_UNITS = ((1, 1, 2), (2, 1, 1))
DOWN_UNITS = (2, 3, 4, 4, 3)
PIECES_EARLY = 1


def dot_nn(left, right):
    return jnp.dot(left, right, preferred_element_type=jnp.float32)


def dot_nt(left, right):
    return lax.dot_general(
        left, right, (((1,), (1,)), ((), ())), preferred_element_type=jnp.float32
    )


def dot_tn(left, right):
    return lax.dot_general(
        left, right, (((0,), (0,)), ((), ())), preferred_element_type=jnp.float32
    )


def layer_kernel(
    sp_count,
    tp_count,
    capacity,
    return_cuts,
    fwd_hbm,
    bwd_hbm,
    k_hbm,
    v_hbm,
    table_hbm,
    q_hbm,
    out_gate_hbm,
    gain_hbm,
    stream_hbm,
    routes_hbm,
    route_weight_hbm,
    mix_gain_hbm,
    ffn_gain_hbm,
    moe_gain_hbm,
    proj_hbm,
    gate_hbm,
    up_hbm,
    down_hbm,
    shared_gate_hbm,
    shared_up_hbm,
    shared_down_hbm,
    out_ref,
    fwd_ref,
    bwd_ref,
    k_ref,
    v_ref,
    table_ref,
    q_ref,
    out_gate_ref,
    gain_ref,
    stream_ref,
    routes_ref,
    route_weight_ref,
    mix_gain_ref,
    ffn_gain_ref,
    moe_gain_ref,
    proj_ref,
    gate_ref,
    up_ref,
    down_ref,
    sgate_ref,
    sup_ref,
    sdown_ref,
    own_ref,
    got_ref,
    mixed_ref,
    land_ref,
    within_ref,
    key_ref,
    sums_f,
    sums_b,
    heads_ref,
    wide_ref,
    residual_ref,
    normed_ref,
    outgoing_ref,
    arrived_ref,
    silu_ref,
    hidden_ref,
    done_ref,
    back_ref,
    local_sem,
    sum_send,
    sum_recv,
    row_send,
    row_recv,
    block_send,
    block_recv,
    back_send,
    back_recv,
    weight_sem,
    pair_send,
    pair_recv,
    cross_send,
    cross_recv,
    relay_send,
    relay_recv,
    near_send,
    near_recv,
    slice_send,
    slice_recv,
    spread_send,
    spread_recv,
    last_send,
    last_recv,
):
    span, lanes = q_ref.shape
    width = v_ref.shape[1]
    heads = lanes // KEY_CHANNELS
    blocks = span // BLK
    tokens = span // tp_count
    model = stream_ref.shape[1]
    part_width = gate_hbm.shape[2]
    slots = sp_count * capacity
    unit = model // sum(DOWN_UNITS)
    depth = model // sum(DEPTH_UNITS[0])
    sp_me = lax.axis_index("sp")
    tp_me = lax.axis_index("tp")
    ranks = tp_count // 2
    rank = lax.div(tp_me, 2)
    seat = lax.rem(tp_me, 2)
    buddy = (sp_me, tp_me + 1 - 2 * seat)
    team = min(8, sp_count)
    place = lax.rem(sp_me, team)
    team_base = sp_me - place
    drains = []

    def sp_peer(step):
        return (lax.rem(sp_me + step, sp_count), tp_me)

    def tp_peer(step):
        return (sp_me, lax.rem(tp_me + step, tp_count))

    def flip(index, mask):
        result, bit = index, 1
        while bit <= mask:
            if mask & bit:
                result = result + bit * (1 - 2 * lax.rem(lax.div(index, bit), 2))
            bit = 2 * bit
        return result

    def mate(distance):
        return (flip(sp_me, distance), tp_me)

    def cross_tp(step):
        return lax.rem(rank + step, ranks) * 2 + seat

    def remote(source, target, send_sem, recv_sem, device):
        return pltpu.make_async_remote_copy(
            src_ref=source,
            dst_ref=target,
            send_sem=send_sem,
            recv_sem=recv_sem,
            device_id=device,
            device_id_type=MESH,
        )

    def send(source, target, send_sem, recv_sem, device):
        copy = remote(source, target, send_sem, recv_sem, device)
        copy.start()
        return copy

    def wait_bytes(ref, semaphore):
        remote(ref, ref, semaphore, semaphore, buddy).wait_recv()

    def sent_bytes(ref, semaphore):
        drains.append(remote(ref, ref, semaphore, semaphore, buddy))

    def fetch(source, target, semaphore):
        copy = pltpu.make_async_copy(source, target, semaphore)
        copy.start()
        return copy

    barrier = pltpu.get_barrier_semaphore()
    for step in range(1, sp_count):
        pl.semaphore_signal(barrier, inc=1, device_id=sp_peer(step), device_id_type=MESH)
    for step in range(1, tp_count):
        pl.semaphore_signal(barrier, inc=1, device_id=tp_peer(step), device_id_type=MESH)
    inputs = [
        fetch(source, target, local_sem.at[at])
        for at, (source, target) in enumerate(
            (
                (fwd_hbm, fwd_ref),
                (bwd_hbm, bwd_ref),
                (k_hbm, k_ref),
                (v_hbm, v_ref),
                (table_hbm, table_ref),
                (q_hbm, q_ref),
                (out_gate_hbm, out_gate_ref),
                (gain_hbm, gain_ref),
                (stream_hbm, stream_ref),
                (routes_hbm, routes_ref),
                (route_weight_hbm, route_weight_ref),
                (mix_gain_hbm, mix_gain_ref),
                (ffn_gain_hbm, ffn_gain_ref),
                (moe_gain_hbm, moe_gain_ref),
            )
        )
    ]

    pieces = [(kind, at) for kind in range(2) for at in range(len(DEPTH_UNITS[kind]))]
    first_down = len(pieces)
    pieces = pieces + [(2, at) for at in range(len(DOWN_UNITS))]
    count = len(pieces)
    groups = [(0, 0), (1, 0)] + [(2, at) for at in range(len(DOWN_UNITS))]

    def columns(first, last, origin=0):
        start = sum(DOWN_UNITS[origin:first]) * unit
        return pl.ds(start, sum(DOWN_UNITS[first:last]) * unit)


    def group_of(index):
        kind, at = pieces[index]
        return 2 + at if kind == 2 else kind

    def group_source(group):
        kind, at = groups[group]
        if kind < 2:
            return (gate_hbm, up_hbm)[kind].at[0]
        return down_hbm.at[0, :, columns(at, at + 1)]

    def group_slot(group, owner):
        kind, at = groups[group]
        if kind < 2:
            return (gate_ref, up_ref)[kind].at[owner]
        row = pl.multiple_of(owner * part_width, part_width)
        return down_ref[at].at[pl.ds(row, part_width), :]

    def weight_slot(index, owner):
        kind, at = pieces[index]
        if kind < 2:
            units = DEPTH_UNITS[kind]
            rows = pl.ds(sum(units[:at]) * depth, units[at] * depth)
            return (gate_ref, up_ref)[kind].at[owner, rows, :]
        return group_slot(group_of(index), owner)

    shared_lanes = shared_gate_hbm.shape[1]

    def shared_slot(kind, owner, which=None):
        if kind < 2:
            ref = (sgate_ref, sup_ref)[kind].at[owner]
            size = model // team
        else:
            row = pl.multiple_of(owner * shared_lanes, shared_lanes)
            ref = sdown_ref.at[pl.ds(row, shared_lanes), :]
            size = shared_lanes // team
        if which is None:
            return ref
        return ref.at[pl.ds(pl.multiple_of(which * size, size), size), :]

    def shared_source(kind, which=None):
        ref = (shared_gate_hbm, shared_up_hbm, shared_down_hbm)[kind]
        if which is None:
            return ref
        size = (shared_lanes if kind == 2 else model) // team
        return ref.at[pl.ds(pl.multiple_of(which * size, size), size), :]

    shared_fetches = [
        fetch(shared_source(kind), shared_slot(kind, tp_me), local_sem.at[len(inputs) + kind])
        for kind in range(3)
    ]
    weight_fetches = [
        fetch(group_source(group), group_slot(group, tp_me), weight_sem.at[group])
        for group in range(len(groups))
    ]

    inputs.append(fetch(proj_hbm, proj_ref, local_sem.at[len(inputs) + 3]))

    row = lax.broadcasted_iota(jnp.int32, (BLK, BLK), 0)
    column = lax.broadcasted_iota(jnp.int32, (BLK, BLK), 1)
    lower = row >= column
    upper = row <= column
    lower_ones = lower.astype(jnp.bfloat16)
    upper_ones = upper.astype(jnp.bfloat16)
    from_lane = lax.broadcasted_iota(jnp.int32, (lanes, lanes), 0)
    to_lane = lax.broadcasted_iota(jnp.int32, (lanes, lanes), 1)
    half = KEY_CHANNELS // 2
    partner = jnp.where(lax.rem(to_lane, KEY_CHANNELS) < half, to_lane + half, to_lane - half)
    swap = (from_lane == partner).astype(jnp.bfloat16)
    own_head = (
        lax.broadcasted_iota(jnp.int32, (width, lanes), 0) // DV
        == lax.broadcasted_iota(jnp.int32, (width, lanes), 1) // KEY_CHANNELS
    )
    lane_head = lax.broadcasted_iota(jnp.int32, (BLK, lanes), 1) // KEY_CHANNELS

    def rotated(tensor, block):
        at = pl.ds(BLK + sp_me * blocks + block, 1)
        cos_at, sin_at = table_ref[0, at, :], table_ref[1, at, :]
        cos_row, sin_row = table_ref[0, 0:BLK, :], table_ref[1, 0:BLK, :]
        cosine = cos_row * cos_at - sin_row * sin_at
        sine = sin_row * cos_at + cos_row * sin_at
        return tensor.astype(jnp.float32) * cosine + dot_nn(tensor, swap) * sine

    def running(ones, raw):
        logs = (jnp.minimum(raw, 0.0) - jnp.log1p(jnp.exp(-jnp.abs(raw)))) * (1.0 / GATE_NORM)
        first = logs.astype(jnp.bfloat16)
        rest = logs - first.astype(jnp.float32)
        second = rest.astype(jnp.bfloat16)
        third = (rest - second.astype(jnp.float32)).astype(jnp.bfloat16)
        return dot_nn(ones, first) + (dot_nn(ones, second) + dot_nn(ones, third))

    pl.semaphore_wait(barrier, sp_count - 1 + tp_count - 1)

    near, slices = [], []
    for kind in range(3):
        for step in range(1, ranks):
            slices.append(
                send(
                    shared_source(kind, place),
                    shared_slot(kind, tp_me, place),
                    slice_send.at[step - 1, kind],
                    slice_recv.at[step - 1, kind],
                    (sp_me, cross_tp(step)),
                )
            )

    crossings = {}
    whole = (gate_hbm.at[0], up_hbm.at[0], down_hbm.at[0])

    fetched = set()

    def cross(index):
        kind, group = pieces[index][0], group_of(index)
        if group not in fetched:
            fetched.add(group)
            weight_fetches[group].wait()
        crossings[index] = [
            send(
                weight_slot(index, tp_me),
                weight_slot(index, tp_me),
                cross_send.at[step - 1, kind],
                cross_recv.at[step - 1, index],
                (sp_me, cross_tp(step)),
            )
            for step in range(1, ranks)
        ]

    def relay(index):
        kind = pieces[index][0]
        for step in range(1, ranks):
            crossings[index][step - 1].wait_recv()
            owner = lax.rem(rank + ranks - step, ranks) * 2 + seat
            send(
                weight_slot(index, owner),
                weight_slot(index, owner),
                relay_send.at[step - 1, kind],
                relay_recv.at[step - 1, group_of(index)],
                buddy,
            )

    for kind in range(3):
        sent_bytes(whole[kind], pair_send.at[kind])
        for step in range(1, ranks):
            sent_bytes(whole[kind], cross_send.at[step - 1, kind])
            sent_bytes(whole[kind], relay_send.at[step - 1, kind])

    for index in range(PIECES_EARLY):
        cross(index)
    for copy in inputs[:5]:
        copy.wait()
    cumul_f, cumul_b, decay_f, decay_b = [], [], [], []
    for block in range(blocks):
        rows = pl.ds(block * BLK, BLK)
        total_f = running(lower_ones, fwd_ref[rows, :])
        total_b = running(upper_ones, bwd_ref[rows, :])
        last_f = total_f[BLK - 1 : BLK]
        last_b = total_b[0:1]
        keys = rotated(k_ref[rows, :], block)
        key_ref[rows, :] = keys
        value_rows = v_ref[rows, :]
        out_f = (keys * jnp.exp(last_f - total_f)).astype(jnp.bfloat16)
        out_b = (keys * jnp.exp(last_b - total_b)).astype(jnp.bfloat16)
        sums_f[block] = jnp.where(own_head, dot_tn(value_rows, out_f), 0.0)
        sums_b[block] = jnp.where(own_head, dot_tn(value_rows, out_b), 0.0)
        cumul_f.append(total_f)
        cumul_b.append(total_b)
        decay_f.append(jnp.exp(last_f))
        decay_b.append(jnp.exp(last_b))

    def packed(total):
        return sum(total[h * DV : (h + 1) * DV] for h in range(heads))

    total = sums_f[0]
    through = decay_f[0]
    for block in range(1, blocks):
        total = total * decay_f[block] + sums_f[block]
        through = through * decay_f[block]
    own_ref[0, 0:DV, :] = packed(total).astype(jnp.bfloat16)
    own_ref[0, DV : DV + 16, :] = jnp.broadcast_to(through, (16, lanes)).astype(jnp.bfloat16)
    total = sums_b[blocks - 1]
    through = decay_b[blocks - 1]
    for block in range(blocks - 2, -1, -1):
        total = total * decay_b[block] + sums_b[block]
        through = through * decay_b[block]
    own_ref[1, 0:DV, :] = packed(total).astype(jnp.bfloat16)
    own_ref[1, DV : DV + 16, :] = jnp.broadcast_to(through, (16, lanes)).astype(jnp.bfloat16)

    for step in range(1, sp_count):
        send(
            own_ref.at[lax.div(sp_me + step, sp_count)],
            got_ref.at[step],
            sum_send.at[0],
            sum_recv.at[0],
            sp_peer(step),
        )
    others = pl.ds(1, sp_count - 1)
    sent_bytes(got_ref.at[others], sum_send.at[0])
    inputs[5].wait()
    query_f, query_b = [], []
    for block in range(blocks):
        rows = pl.ds(block * BLK, BLK)
        queries = rotated(q_ref[rows, :], block) * KEY_CHANNELS ** (-0.5)
        keys = key_ref[rows, :]
        total_f, total_b = cumul_f[block], cumul_b[block]
        middle_f = total_f[BLK // 2 - 1 : BLK // 2]
        middle_b = total_b[BLK // 2 : BLK // 2 + 1]
        scaled_qf = queries * jnp.exp(total_f - middle_f)
        scaled_qb = queries * jnp.exp(total_b - middle_b)
        scaled_kf = (keys * jnp.exp(middle_f - total_f)).astype(jnp.bfloat16)
        scaled_kb = (keys * jnp.exp(middle_b - total_b)).astype(jnp.bfloat16)
        query_f.append((queries * jnp.exp(total_f)).astype(jnp.bfloat16))
        query_b.append((queries * jnp.exp(total_b)).astype(jnp.bfloat16))
        for h in range(heads):
            mine = lane_head == h
            scores_f = dot_nt(jnp.where(mine, scaled_qf, 0.0).astype(jnp.bfloat16), scaled_kf)
            scores_b = dot_nt(jnp.where(mine, scaled_qb, 0.0).astype(jnp.bfloat16), scaled_kb)
            scores = jnp.where(lower, scores_f, 0.0) + jnp.where(upper, scores_b, 0.0)
            within_ref[rows, h * DV : (h + 1) * DV] = dot_nn(
                scores.astype(jnp.bfloat16), v_ref[rows, h * DV : (h + 1) * DV]
            )
    wait_bytes(got_ref.at[others], sum_recv.at[0])
    carry_f = jnp.zeros((DV, lanes), jnp.float32)
    carry_b = jnp.zeros((DV, lanes), jnp.float32)
    for step in range(sp_count - 1, 0, -1):
        state = got_ref[step, 0:DV, :].astype(jnp.float32)
        through = got_ref[step, DV : DV + 16, :].astype(jnp.float32)[0:1]
        carry_f = jnp.where(step <= sp_me, carry_f * through + state, carry_f)
    for step in range(1, sp_count):
        state = got_ref[step, 0:DV, :].astype(jnp.float32)
        through = got_ref[step, DV : DV + 16, :].astype(jnp.float32)[0:1]
        carry_b = jnp.where(step > sp_me, carry_b * through + state, carry_b)

    def unpacked(carry):
        return jnp.where(own_head, jnp.concatenate([carry] * heads, axis=0), 0.0)

    state = unpacked(carry_f)
    for block in range(blocks):
        rows = pl.ds(block * BLK, BLK)
        within_ref[rows, :] += dot_nt(query_f[block], state.astype(jnp.bfloat16))
        if block < blocks - 1:
            state = state * decay_f[block] + sums_f[block]
    inputs[6].wait()
    inputs[7].wait()
    state = unpacked(carry_b)
    for block in range(blocks - 1, -1, -1):
        rows = pl.ds(block * BLK, BLK)
        attended = within_ref[rows, :] + dot_nt(query_b[block], state.astype(jnp.bfloat16))
        if block > 0:
            state = state * decay_b[block] + sums_b[block]
        for h in range(heads):
            part = attended[:, h * DV : (h + 1) * DV]
            square = jnp.mean(part * part, axis=-1, keepdims=True)
            gate = out_gate_ref[rows, h * DV : (h + 1) * DV].astype(jnp.float32)
            mixed_ref[rows, h * DV : (h + 1) * DV] = (
                part
                * lax.rsqrt(square + EPS)
                * gain_ref[:, h * DV : (h + 1) * DV]
                * (gate / (1.0 + jnp.exp(-gate)))
            ).astype(jnp.bfloat16)

    row_copies = []
    for step in range(1, tp_count):
        target = lax.rem(tp_me + step, tp_count)
        row_copies.append(
            send(
                mixed_ref.at[pl.ds(pl.multiple_of(target * tokens, tokens), tokens)],
                land_ref.at[tp_me],
                row_send.at[0],
                row_recv.at[step],
                (sp_me, target),
            )
        )
    sent_bytes(mixed_ref.at[pl.ds(0, (tp_count - 1) * tokens)], row_send.at[0])
    for index in range(PIECES_EARLY, count):
        cross(index)
    spread_masks = [0]
    spread_copies = slices
    spread_count = 0

    def spread(bit):
        nonlocal spread_masks, spread_copies, spread_count
        for copy in spread_copies:
            copy.wait_recv()
        spread_copies = []
        for mask in spread_masks:
            which = flip(place, mask)
            for step in range(1, ranks):
                owner = lax.rem(rank + ranks - step, ranks) * 2 + seat
                for kind in range(3):
                    spread_copies.append(
                        send(
                            shared_slot(kind, owner, which),
                            shared_slot(kind, owner, which),
                            spread_send.at[step - 1, kind],
                            spread_recv.at[step - 1, spread_count, kind],
                            mate(bit),
                        )
                    )
            spread_count += 1
        spread_masks = spread_masks + [mask + bit for mask in spread_masks]

    stages = [team >> shift for shift in range(1, team.bit_length())]
    spread(stages[0])
    land_ref[tp_me] = mixed_ref[pl.ds(pl.multiple_of(tp_me * tokens, tokens), tokens), :]

    for copy in inputs[8:]:
        copy.wait()
    token_row = lax.broadcasted_iota(jnp.int32, (tokens, tokens), 0)
    token_column = lax.broadcasted_iota(jnp.int32, (tokens, tokens), 1)
    earlier = (token_row < token_column).astype(jnp.bfloat16)
    expert_row = lax.broadcasted_iota(jnp.int32, (max(8, sp_count), tokens), 0)
    choices = [routes_ref[choice : choice + 1, :] for choice in range(TOPK)]
    named = [(chosen == expert_row).astype(jnp.float32) for chosen in choices]
    before = dot_nn(sum(named).astype(jnp.bfloat16), earlier)
    slot_row = lax.broadcasted_iota(jnp.int32, (slots, tokens), 0)
    weights = jnp.zeros((slots, tokens), jnp.float32)
    picked = jnp.zeros((slots, tokens), jnp.float32)
    for choice in range(TOPK):
        slot = jnp.sum(before * named[choice], axis=0, keepdims=True).astype(jnp.int32)
        distance = lax.bitwise_xor(choices[choice], jnp.full((1, tokens), sp_me, jnp.int32))
        hit = slot_row == distance * capacity + slot
        picked = jnp.where(hit, 1.0, picked)
        weights = jnp.where(hit, route_weight_ref[choice : choice + 1, :], weights)
    picked = picked.astype(jnp.bfloat16)
    weights = jnp.transpose(weights)
    weights_high = weights.astype(jnp.bfloat16)
    weights_low = (weights - weights_high.astype(jnp.float32)).astype(jnp.bfloat16)

    for copy in row_copies:
        copy.wait_recv()
    for source in range(tp_count):
        heads_ref[:, source * width : (source + 1) * width] = land_ref[source]
    square = jnp.zeros((tokens, 1), jnp.float32)
    for at in range(0, model, 512):
        part = dot_nn(heads_ref[...], proj_ref[:, at : at + 512])
        wide_ref[:, at : at + 512] = part
        square = square + jnp.sum(part * part, axis=-1, keepdims=True)
    scale = lax.rsqrt(square * (1.0 / model) + EPS)
    square = jnp.zeros((tokens, 1), jnp.float32)
    for at in range(0, model, 512):
        part = (
            stream_ref[:, at : at + 512].astype(jnp.float32)
            + wide_ref[:, at : at + 512] * scale * mix_gain_ref[:, at : at + 512]
        ).astype(jnp.bfloat16)
        residual_ref[:, at : at + 512] = part
        part = part.astype(jnp.float32)
        square = square + jnp.sum(part * part, axis=-1, keepdims=True)
    scale = lax.rsqrt(square * (1.0 / model) + EPS)
    for at in range(0, model, 512):
        part = (
            residual_ref[:, at : at + 512].astype(jnp.float32)
            * scale
            * ffn_gain_ref[:, at : at + 512]
        ).astype(jnp.bfloat16)
        normed_ref[:, at : at + 512] = part
        outgoing_ref[:, :, at : at + 512] = (
            dot_nn(picked, part).astype(jnp.bfloat16).reshape(sp_count, capacity, 512)
        )

    far = sp_count // 2
    order = list(range(far, sp_count)) + list(range(1, far))
    for distance in order:
        send(
            outgoing_ref.at[distance],
            arrived_ref.at[distance],
            block_send.at[0],
            block_recv.at[distance // far],
            mate(distance),
        )
    sent_bytes(outgoing_ref.at[others], block_send.at[0])
    for bit in stages[1:-1]:
        spread(bit)
    arrived_ref[0] = outgoing_ref[0]
    for kind in range(3):
        near.append(
            send(
                shared_source(kind),
                shared_slot(kind, tp_me),
                near_send.at[kind],
                near_recv.at[kind],
                buddy,
            )
        )
    pairs = [
        send(
            group_slot(group, tp_me) if group in fetched else group_source(group),
            group_slot(group, tp_me),
            pair_send.at[groups[group][0]],
            pair_recv.at[group],
            buddy,
        )
        for group in range(len(groups))
    ]


    for index in range(PIECES_EARLY):
        relay(index)

    def arrive(group):
        pairs[group].wait_recv()
        for step in range(1, ranks):
            owner = lax.rem(rank + ranks - step, ranks) * 2 + 1 - seat
            wait_bytes(group_slot(group, owner), relay_recv.at[step - 1, group])

    def put_hidden(owner, low, high, values):
        lane = owner * part_width
        hidden_ref[low * capacity : high * capacity, lane : lane + part_width] = values.astype(
            jnp.bfloat16
        )

    middle = first_down // 2
    for index in range(PIECES_EARLY, middle):
        relay(index)
    if len(stages) > 1:
        spread(stages[-1])
    for index in range(middle, first_down - 2):
        relay(index)
    arrive(0)

    def wait_blocks(low, high):
        inner = pl.ds(max(low, 1), high - max(low, 1))
        if high > max(low, 1):
            wait_bytes(arrived_ref.at[inner], block_recv.at[low // far])

    def rows_of(low, high):
        return arrived_ref[low:high].reshape((high - low) * capacity, model)

    per_cut = len(DOWN_UNITS) // return_cuts

    def give_back(part, low, high):
        for at in range(part * per_cut, (part + 1) * per_cut):
            inner = columns(at, at + 1, part * per_cut)
            done_ref[part][low:high, :, inner] = (
                dot_nn(hidden_ref[low * capacity : high * capacity, :], down_ref[at][...])
                .astype(jnp.bfloat16)
                .reshape(high - low, capacity, inner.size)
            )
        for distance in order:
            if low <= distance < high:
                send(
                    done_ref[part].at[distance],
                    back_ref[part].at[distance],
                    back_send.at[0],
                    back_recv.at[part],
                    mate(distance),
                )

    def down_ready(part):
        for at in range(part * per_cut, (part + 1) * per_cut):
            relay(first_down + at)
            arrive(2 + at)

    wait_blocks(far, sp_count)
    rows = rows_of(far, sp_count)
    for owner in range(tp_count):
        lane = owner * part_width
        silu_ref[:, lane : lane + part_width] = jax.nn.silu(dot_nn(rows, gate_ref[owner]))
    relay(first_down - 2)
    relay(first_down - 1)
    arrive(1)
    for owner in range(tp_count):
        lane = owner * part_width
        values = silu_ref[:, lane : lane + part_width] * dot_nn(rows, up_ref[owner])
        put_hidden(owner, far, sp_count, values)
    down_ready(0)
    give_back(0, far, sp_count)
    wait_blocks(0, far)
    rows = rows_of(0, far)
    for owner in range(tp_count):
        values = jax.nn.silu(dot_nn(rows, gate_ref[owner])) * dot_nn(rows, up_ref[owner])
        put_hidden(owner, 0, far, values)
    give_back(0, 0, far)
    for part in range(1, return_cuts):
        down_ready(part)
        give_back(part, 0, sp_count)
    for part in range(return_cuts):
        back_ref[part][0] = done_ref[part][0]
    sent_bytes(outgoing_ref.at[others], back_send.at[0])

    for copy in spread_copies:
        copy.wait_recv()
    lasts = []
    for step in range(1, ranks):
        owner = lax.rem(rank + ranks - step, ranks) * 2 + seat
        for kind in range(3):
            lasts.append(
                send(
                    shared_slot(kind, owner),
                    shared_slot(kind, owner),
                    last_send.at[step - 1, kind],
                    last_recv.at[step - 1, kind],
                    buddy,
                )
            )
    for copy in shared_fetches:
        copy.wait()
    for copy in near + lasts:
        copy.wait_recv()
    shared_hidden = jnp.concatenate(
        [
            jax.nn.silu(dot_nn(normed_ref[...], sgate_ref[owner]))
            * dot_nn(normed_ref[...], sup_ref[owner])
            for owner in range(tp_count)
        ],
        axis=1,
    ).astype(jnp.bfloat16)
    for at in range(0, model, 512):
        wide_ref[:, at : at + 512] = dot_nn(shared_hidden, sdown_ref[:, at : at + 512])

    square = jnp.zeros((tokens, 1), jnp.float32)
    for part in range(return_cuts):
        wait_bytes(back_ref[part].at[others], back_recv.at[part])
        inner = columns(part * per_cut, (part + 1) * per_cut)
        back = back_ref[part][...].reshape(slots, inner.size)
        mixture = wide_ref[:, inner] + dot_nn(weights_high, back) + dot_nn(weights_low, back)
        wide_ref[:, inner] = mixture
        square = square + jnp.sum(mixture * mixture, axis=-1, keepdims=True)
    scale = lax.rsqrt(square * (1.0 / model) + EPS)
    for at in range(0, model, 512):
        out_ref[:, at : at + 512] = (
            residual_ref[:, at : at + 512].astype(jnp.float32)
            + wide_ref[:, at : at + 512] * scale * moe_gain_ref[:, at : at + 512]
        ).astype(out_ref.dtype)
    for kind in range(3):
        size = (shared_lanes if kind == 2 else model) // team * (team - 1)
        ref = (sgate_ref, sup_ref, sdown_ref)[kind]
        for step in range(1, ranks):
            if kind == 2:
                sent_bytes(ref.at[pl.ds(0, size), :], spread_send.at[step - 1, kind])
            else:
                sent_bytes(ref.at[0, pl.ds(0, size), :], spread_send.at[step - 1, kind])
    for copy in slices + near + lasts + drains:
        copy.wait_send()


def body(
    stream,
    queries,
    key_rows,
    values,
    out_gate,
    fwd_decay,
    bwd_decay,
    head_gain,
    out_proj,
    mix_gain,
    ffn_gain,
    moe_gain,
    routes,
    route_weight,
    expert_gate,
    expert_up,
    expert_down,
    shared_gate,
    shared_up,
    shared_down,
):
    sp_count = lax.axis_size("sp")
    tp_count = lax.axis_size("tp")
    tokens, model = stream.shape
    span, lanes = queries.shape
    width = values.shape[1]
    blocks = span // BLK
    part_width = expert_gate.shape[2]
    shared_width = shared_gate.shape[1] * tp_count
    capacity = max(2, 3 * tokens * TOPK // (2 * sp_count))
    capacity = -(-capacity // ROW_TILE) * ROW_TILE
    slots = sp_count * capacity
    return_cuts = len(DOWN_UNITS) if sp_count <= 16 else 1
    unit = model // sum(DOWN_UNITS)
    cuts = [width * unit for width in DOWN_UNITS]
    back_cuts = cuts if return_cuts > 1 else [model]
    team = min(8, sp_count)
    ranks = tp_count // 2

    half = KEY_CHANNELS // 2
    lane = np.arange(lanes) % KEY_CHANNELS
    frequency = ROPE_BASE ** (-(lane % half) / half)
    positions = np.concatenate([np.arange(BLK), np.arange(sp_count * blocks) * BLK])
    angles = positions[:, None] * frequency[None, :]
    sign = np.where(lane < half, -1.0, 1.0)
    table = jnp.asarray(np.stack([np.cos(angles), np.sin(angles) * sign]), jnp.float32)

    vmem = pl.BlockSpec(memory_space=pltpu.VMEM)
    hbm = pl.BlockSpec(memory_space=pl.ANY)
    dma = pltpu.SemaphoreType.DMA
    bf16, f32 = jnp.bfloat16, jnp.float32
    count = sum(len(units) for units in DEPTH_UNITS) + len(DOWN_UNITS)
    groups = 2 + len(DOWN_UNITS)
    inputs = (
        fwd_decay,
        bwd_decay,
        key_rows,
        values,
        table,
        queries,
        out_gate,
        head_gain.reshape(1, -1),
        stream,
        routes.T,
        route_weight.T,
        mix_gain.reshape(1, -1),
        ffn_gain.reshape(1, -1),
        moe_gain.reshape(1, -1),
        out_proj,
    )
    updated = pl.pallas_call(
        functools.partial(layer_kernel, sp_count, tp_count, capacity, return_cuts),
        out_shape=jax.ShapeDtypeStruct(stream.shape, bf16),
        in_specs=[hbm] * (len(inputs) + 6),
        out_specs=vmem,
        scratch_shapes=[
            *(pltpu.VMEM(array.shape, array.dtype) for array in inputs),
            pltpu.VMEM((tp_count, model, part_width), bf16),
            pltpu.VMEM((tp_count, model, part_width), bf16),
            [pltpu.VMEM((tp_count * part_width, cut), bf16) for cut in cuts],
            pltpu.VMEM((tp_count, model, shared_width // tp_count), bf16),
            pltpu.VMEM((tp_count, model, shared_width // tp_count), bf16),
            pltpu.VMEM((shared_width, model), bf16),
            pltpu.VMEM((2, DV + 16, lanes), bf16),
            pltpu.VMEM((sp_count, DV + 16, lanes), bf16),
            pltpu.VMEM((span, width), bf16),
            pltpu.VMEM((tp_count, tokens, width), bf16),
            pltpu.VMEM((span, width), f32),
            pltpu.VMEM((span, lanes), f32),
            pltpu.VMEM((blocks, width, lanes), f32),
            pltpu.VMEM((blocks, width, lanes), f32),
            pltpu.VMEM((tokens, tp_count * width), bf16),
            pltpu.VMEM((tokens, model), f32),
            pltpu.VMEM((tokens, model), bf16),
            pltpu.VMEM((tokens, model), bf16),
            pltpu.VMEM((sp_count, capacity, model), bf16),
            pltpu.VMEM((sp_count, capacity, model), bf16),
            pltpu.VMEM((slots // 2, tp_count * part_width), f32),
            pltpu.VMEM((slots, tp_count * part_width), bf16),
            [pltpu.VMEM((sp_count, capacity, cut), bf16) for cut in back_cuts],
            [pltpu.VMEM((sp_count, capacity, cut), bf16) for cut in back_cuts],
            dma((len(inputs) + 3,)),
            dma((1,)),
            dma((1,)),
            dma((1,)),
            dma((tp_count,)),
            dma((1,)),
            dma((2,)),
            dma((1,)),
            dma((return_cuts,)),
            dma((groups,)),
            dma((3,)),
            dma((groups,)),
            dma((ranks - 1, 3)),
            dma((ranks - 1, count)),
            dma((ranks - 1, 3)),
            dma((ranks - 1, groups)),
            dma((3,)),
            dma((3,)),
            dma((ranks - 1, 3)),
            dma((ranks - 1, 3)),
            dma((ranks - 1, 3)),
            dma((ranks - 1, team - 1, 3)),
            dma((ranks - 1, 3)),
            dma((ranks - 1, 3)),
        ],
        compiler_params=pltpu.CompilerParams(
            collective_id=0, has_side_effects=True, vmem_limit_bytes=62 * 2**20
        ),
    )(
        *inputs,
        expert_gate,
        expert_up,
        expert_down,
        shared_gate,
        shared_up,
        shared_down,
    )
    return updated


def solution(mesh):
    return jax.shard_map(
        body,
        mesh=mesh,
        in_specs=(
            P(("sp", "tp"), None),
            P("sp", "tp"),
            P("sp", "tp"),
            P("sp", "tp"),
            P("sp", "tp"),
            P("sp", "tp"),
            P("sp", "tp"),
            P("tp"),
            P(),
            P(),
            P(),
            P(),
            P(("sp", "tp"), None),
            P(("sp", "tp"), None),
            P("sp", None, "tp"),
            P("sp", None, "tp"),
            P("sp", "tp", None),
            P(None, "tp"),
            P(None, "tp"),
            P("tp", None),
        ),
        out_specs=P(("sp", "tp"), None),
        check_vma=False,
    )
```
